256 devices in a mesh: sp: 64 (over z, x, core), tp: 4 (over y).
Axes of the slice: x: 4, y: 4, z: 8, core: 2. Of those that a mesh axis runs over, the one named last changes fastest.
Arguments:
- moe_input: bfloat16 [16384, 2048], P('sp'), may hold values from -6 to 6
- cotangent: bfloat16 [16384, 2048], P('sp'), may hold values from -16 to 16
- expert_ids: int32 [16384, 2], P('sp'), may hold values from 0 to 63, as said below
- route_weights: float32 [16384, 2], P('sp'), may hold values from 0.05 to 1
- gate_weight: bfloat16 [64, 2048, 1024], P('sp', None, 'tp'), may hold values from -0.125 to 0.125
- up_weight: bfloat16 [64, 2048, 1024], P('sp', None, 'tp'), may hold values from -0.125 to 0.125
- down_weight: bfloat16 [64, 1024, 2048], P('sp', 'tp'), may hold values from -0.1875 to 0.1875
- out_weight: bfloat16 [2048, 1024], P(None, 'tp'), may hold values from -0.1875 to 0.1875
- mixer_out: bfloat16 [16384, 1024], P('sp', 'tp'), may hold values from -6 to 6
- query_vectors: bfloat16 [16384, 512], P('sp', 'tp'), may hold values from -0.37109375 to 0.37109375
- key_vectors: bfloat16 [16384, 512], P('sp', 'tp'), may hold values from -0.37109375 to 0.37109375
- value_vectors: bfloat16 [16384, 1024], P('sp', 'tp'), may hold values from -6 to 6
- log_decay: float32 [16384, 512], P('sp', 'tp'), may hold values from -2 to 0
Outputs:
- grad_gate: bfloat16 [64, 2048, 1024], P('sp', None, 'tp')
- grad_up: bfloat16 [64, 2048, 1024], P('sp', None, 'tp')
- grad_down: bfloat16 [64, 1024, 2048], P('sp', 'tp')
- grad_out_weight: float32 [2048, 1024], P('sp', 'tp')
- grad_queries: bfloat16 [16384, 512], P('sp', 'tp')
- grad_keys: bfloat16 [16384, 512], P('sp', 'tp')
- grad_values: bfloat16 [16384, 1024], P('sp', 'tp')
- grad_log_decay: float32 [16384, 512], P('sp', 'tp')
The draws below stay inside these ranges and needn't reach their ends.
Inputs may be any that keep to these rules, and one draw needn't show every extreme that they name: `expert_ids`: each row names two different experts of one group, expert e lying in group e // 16. Each aligned block of 256 rows names every expert exactly 8 times and has equally many rows in each of the 4 groups.
All inputs are finite; a program needn't handle non-finite values.
Results may differ from the reference program's by a relative error of at most 0.01145.
Values may be sent and summed in bfloat16 or wider, within the bound.
A program may use at most 64 MiB of HBM per device.

```python
import math
import jax
import jax.numpy as jnp
from jax import lax

D = 2048
ATTENTION_HEADS = 8
KEY_CHANNELS = 64
VAL_DIM = 128
EXP_HIDDEN = 1024
GROUPS = 4
BLOCK = 64
TOK_DEV = 256
SEQUENCE_TOKENS = 16384
EXPERTS = 64
KEY_WIDTH = 512
VAL_WIDTH = 1024
N_TP = 4


def draw_expert_ids(key, part):
    block_total = SEQUENCE_TOKENS // TOK_DEV
    per_group = EXPERTS // GROUPS
    block_keys = jax.random.split(key, block_total)

    def one_block(block_key):
        keys_here = jax.random.split(block_key, 3)
        shuffled = jax.random.permutation(keys_here[0], TOK_DEV).astype(jnp.int32)
        group_of = shuffled % GROUPS
        rank_of = shuffled // GROUPS
        shifts = jax.random.randint(keys_here[1], (GROUPS,), 0, per_group)
        offsets = jax.random.randint(keys_here[2], (GROUPS,), 0, per_group - 1)
        first_pick = (rank_of + shifts[group_of]) % per_group
        second_pick = (first_pick + 1 + offsets[group_of]) % per_group
        return jnp.stack([group_of * per_group + first_pick, group_of * per_group + second_pick], axis=1)
    return jax.vmap(one_block)(block_keys).reshape(SEQUENCE_TOKENS, 2).astype(jnp.int32)


def draw_log_decay(key, part):
    channels = ATTENTION_HEADS * KEY_CHANNELS
    block_total = SEQUENCE_TOKENS // TOK_DEV
    key_sequence = jax.random.split(key, 7)
    fast_share = 0.5
    fast_mask = jax.random.uniform(key_sequence[0], (channels,)) < fast_share
    slow_rate = jnp.exp(jax.random.uniform(key_sequence[1], (channels,), minval=math.log(0.05), maxval=math.log(0.3))) / SEQUENCE_TOKENS
    fast_rate = jnp.exp(jax.random.uniform(key_sequence[2], (channels,), minval=math.log(0.01), maxval=math.log(1.0 / 30.0)))
    baseline_rate = jnp.where(fast_mask, fast_rate, slow_rate)
    hardware_factor = jnp.exp(jax.random.uniform(key_sequence[3], (block_total,), minval=math.log(0.5), maxval=math.log(2.0)))
    hardware_factor = jnp.repeat(hardware_factor, TOK_DEV)
    random_noise = 1.0 + 0.5 * jax.random.uniform(key_sequence[4], (SEQUENCE_TOKENS, channels), minval=-1.0, maxval=1.0)
    spike_locations = jax.random.randint(key_sequence[5], (2, ATTENTION_HEADS), 0, SEQUENCE_TOKENS)
    spike_size = jax.random.uniform(key_sequence[6], (2, ATTENTION_HEADS), minval=math.log(0.6), maxval=math.log(0.8))
    token_positions = jnp.arange(SEQUENCE_TOKENS, dtype=jnp.int32)
    spike_hits = (token_positions[:, None, None] == spike_locations[None, :, :]).astype(jnp.float32)
    spike_events = jnp.sum(spike_hits * spike_size[None, :, :], axis=1)
    spike_events = jnp.repeat(spike_events, KEY_CHANNELS, axis=1)
    return (spike_events - baseline_rate[None, :] * hardware_factor[:, None] * random_noise).astype(jnp.float32)


def spiked(array, key, source, target, shards_of, factor):
    owner, partner = [(jnp.arange(array.shape[position]) // (array.shape[position] // shards_of)).reshape([-1 if axis == position else 1 for axis in range(array.ndim)]) for position in (source, target)]
    chosen = jax.random.permutation(key, shards_of)[partner]
    strong = (owner == chosen) | (owner == (partner + shards_of // 2) % shards_of)
    return jnp.where(strong, factor * array, array)


def levels(own_key, shape, shards, least, high):
    def one(dim, shards_of):
        draws = jax.random.uniform(jax.random.fold_in(jax.random.fold_in(own_key, 6), dim), (shards_of,), jnp.float32, least / len(shards), high / len(shards))
        return jnp.repeat(jnp.exp(draws), shape[dim] // shards_of).reshape((-1,) + (1,) * (len(shape) - dim - 1))

    factor_of = one(*shards[0])
    for cut in shards[1:]:
        factor_of = factor_of * one(*cut)
    return factor_of


def bell_draw(rng, shape, scale, limit, shards=(), kind=jnp.bfloat16):
    factor_of = levels(rng, shape, shards, -0.22, 0.18) if shards else 1.0
    entries = jax.random.normal(rng, shape, jnp.float32) * scale * factor_of
    return jnp.minimum(jnp.maximum(entries, -limit), limit).astype(kind)


def gaussian_with(stream_key, extent, deviation, most, pieces, heavy, kind=jnp.bfloat16):
    entries = deviation * jax.random.normal(stream_key, extent, jnp.float32)
    if pieces:
        entries = entries * levels(stream_key, extent, pieces, -0.22, 0.18)
    return jnp.clip(spiked(entries, jax.random.fold_in(stream_key, 3), *heavy), -most, most).astype(kind)


def setup_inputs(seed: int = 0) -> dict:
    key_list = jax.random.split(jax.random.key(seed), 14)
    return {
        "moe_input": bell_draw(key_list[0], (SEQUENCE_TOKENS, D), 1.0, 6.0, ((0, 64),)),
        "cotangent": gaussian_with(key_list[1], (SEQUENCE_TOKENS, D), 1.0, 16.0, ((0, 64),), (0, 1, 64, 4.0)),
        "expert_ids": draw_expert_ids(jax.random.fold_in(key_list[13], 71), 0),
        "route_weights": jnp.clip(0.05 + 0.95 * jax.random.uniform(key_list[3], (SEQUENCE_TOKENS, 2), jnp.float32) ** levels(key_list[3], (SEQUENCE_TOKENS, 2), ((0, 64),), -0.2, 0.2), 0.05, 1.0),
        "gate_weight": bell_draw(key_list[4], (EXPERTS, D, EXP_HIDDEN), D ** -0.5, 0.125, ((0, 64), (2, 4))),
        "up_weight": bell_draw(key_list[5], (EXPERTS, D, EXP_HIDDEN), D ** -0.5, 0.125, ((0, 64), (2, 4))),
        "down_weight": bell_draw(key_list[6], (EXPERTS, EXP_HIDDEN, D), EXP_HIDDEN ** -0.5, 0.1875, ((0, 64), (1, 4))),
        "out_weight": bell_draw(key_list[7], (D, VAL_WIDTH), VAL_WIDTH ** -0.5, 0.1875, ((1, 4),)),
        "mixer_out": bell_draw(key_list[8], (SEQUENCE_TOKENS, VAL_WIDTH), 1.0, 6.0, ((0, 64), (1, 4))),
        "query_vectors": bell_draw(key_list[9], (SEQUENCE_TOKENS, KEY_WIDTH), (0.7 * SEQUENCE_TOKENS ** -0.25), 0.37109375, ((0, 64), (1, 4))),
        "key_vectors": bell_draw(key_list[10], (SEQUENCE_TOKENS, KEY_WIDTH), (0.7 * SEQUENCE_TOKENS ** -0.25), 0.37109375, ((0, 64), (1, 4))),
        "value_vectors": bell_draw(key_list[11], (SEQUENCE_TOKENS, VAL_WIDTH), 1.0, 6.0, ((0, 64), (1, 4))),
        "log_decay": draw_log_decay(jax.random.fold_in(key_list[13], 71), 0),
    }


HIGHEST = lax.Precision.HIGHEST

def block_step(memory, inputs):
    query_block, key_block, value_block, decay_block = inputs
    block_len = query_block.shape[1]
    causal = jnp.tril(jnp.ones((block_len, block_len), dtype=bool))
    cumulative = jnp.cumsum(decay_block, axis=1)
    carried = jnp.einsum('hcd,hdv->hcv', query_block * jnp.exp(cumulative), memory, precision=HIGHEST)
    difference = cumulative[:, :, None, :] - cumulative[:, None, :, :]
    decay = jnp.exp(jnp.where(causal[None, :, :, None], difference, -jnp.inf))
    scores = jnp.einsum('htd,hsd,htsd->hts', query_block, key_block, decay, precision=HIGHEST)
    within = jnp.einsum('hts,hsv->htv', scores, value_block, precision=HIGHEST)
    final_row = cumulative[:, -1:, :]
    memory = jnp.exp(final_row[:, 0, :])[:, :, None] * memory + jnp.einsum('hsd,hsv->hdv', key_block * jnp.exp(final_row - cumulative), value_block, precision=HIGHEST)
    return (memory, carried + within)

def run_blocks(query_heads, key_heads, value_heads, decay_heads, memory):
    head_count = query_heads.shape[0]
    length = query_heads.shape[1]
    block_count = length // BLOCK

    def to_blocks(matrix):
        return matrix.reshape(head_count, block_count, BLOCK, matrix.shape[-1]).transpose(1, 0, 2, 3)
    memory, outputs = lax.scan(jax.checkpoint(block_step), memory, (to_blocks(query_heads), to_blocks(key_heads), to_blocks(value_heads), to_blocks(decay_heads)))
    return (outputs.transpose(1, 0, 2, 3).reshape(head_count, length, outputs.shape[-1]), memory)

def expert_backward(inputs):
    routed, routed_cot, gate_local, up_local, down_local = inputs
    pre_gate = jnp.dot(routed, gate_local, preferred_element_type=jnp.float32)
    pre_up = jnp.dot(routed, up_local, preferred_element_type=jnp.float32)
    sigmoid_gate = jax.nn.sigmoid(pre_gate)
    activated = pre_gate * sigmoid_gate
    hidden = (activated * pre_up).astype(jnp.bfloat16)
    delta_hidden = jnp.dot(routed_cot, down_local.T, preferred_element_type=jnp.float32)
    grad_down = jnp.dot(hidden.T, routed_cot, preferred_element_type=jnp.float32).astype(jnp.bfloat16)
    delta_gate = (delta_hidden * pre_up * sigmoid_gate * (1.0 + pre_gate * (1.0 - sigmoid_gate))).astype(jnp.bfloat16)
    delta_up = (delta_hidden * activated).astype(jnp.bfloat16)
    grad_gate = jnp.dot(routed.T, delta_gate, preferred_element_type=jnp.float32).astype(jnp.bfloat16)
    grad_up = jnp.dot(routed.T, delta_up, preferred_element_type=jnp.float32).astype(jnp.bfloat16)
    unit_span = gate_local.shape[1] // N_TP
    summed = jnp.zeros((routed.shape[0], routed.shape[1]), jnp.float32)
    for member in range(N_TP):
        lower_unit = member * unit_span
        upper_unit = lower_unit + unit_span
        partial_value = jnp.dot(delta_gate[:, lower_unit:upper_unit], gate_local[:, lower_unit:upper_unit].T, preferred_element_type=jnp.float32)
        partial_value = partial_value + jnp.dot(delta_up[:, lower_unit:upper_unit], up_local[:, lower_unit:upper_unit].T, preferred_element_type=jnp.float32)
        summed = summed + lax.optimization_barrier(partial_value.astype(jnp.bfloat16)).astype(jnp.float32)
    return (grad_gate, grad_up, grad_down, summed.astype(jnp.bfloat16))

def reference(moe_input, cotangent, expert_ids, route_weights, gate_weight, up_weight, down_weight, out_weight, mixer_out, query_vectors, key_vectors, value_vectors, log_decay):
    tok_count = moe_input.shape[0]
    model_width = moe_input.shape[1]
    expert_count = gate_weight.shape[0]
    slot_count = 2 * tok_count // expert_count
    flat_ids = expert_ids.reshape(-1).astype(jnp.int32)
    sorting = jnp.argsort(flat_ids, stable=True).astype(jnp.int32)
    source_rows = (sorting // 2).astype(jnp.int32)
    scaled = (route_weights[:, :, None] * cotangent[:, None, :].astype(jnp.float32)).astype(jnp.bfloat16)
    scaled = scaled.reshape(2 * tok_count, model_width)
    rows_in = moe_input[source_rows].reshape(expert_count, slot_count, model_width)
    rows_cot = scaled[sorting].reshape(expert_count, slot_count, model_width)
    grad_gate, grad_up, grad_down, returned = lax.map(expert_backward, (rows_in, rows_cot, gate_weight, up_weight, down_weight))
    inverse = jnp.argsort(sorting).astype(jnp.int32)
    per_slot = returned.reshape(2 * tok_count, model_width)[inverse].reshape(tok_count, 2, model_width)
    per_slot = per_slot.astype(jnp.float32)
    token_grad = (cotangent.astype(jnp.float32) + per_slot[:, 0] + per_slot[:, 1]).astype(jnp.bfloat16)
    mixer_grad = jnp.dot(token_grad, out_weight, preferred_element_type=jnp.float32).astype(jnp.bfloat16)
    grad_out_weight = jnp.dot(token_grad.T, mixer_out, preferred_element_type=jnp.float32)

    def heads_first(matrix, channel_size):
        return matrix.astype(jnp.float32).reshape(tok_count, ATTENTION_HEADS, channel_size).transpose(1, 0, 2)

    def tokens_first(matrix):
        return matrix.transpose(1, 0, 2).reshape(tok_count, -1)

    def forward(query_in, key_in, value_in, decay_in):
        initial = jnp.zeros((ATTENTION_HEADS, KEY_CHANNELS, VAL_DIM), jnp.float32)
        return run_blocks(query_in * KEY_CHANNELS ** (-0.5), key_in, value_in, decay_in, initial)[0]
    pullback = jax.vjp(forward, heads_first(query_vectors, KEY_CHANNELS), heads_first(key_vectors, KEY_CHANNELS), heads_first(value_vectors, VAL_DIM), heads_first(log_decay, KEY_CHANNELS))[1]
    grads = pullback(heads_first(mixer_grad, VAL_DIM))
    return (grad_gate, grad_up, grad_down, grad_out_weight, tokens_first(grads[0]).astype(jnp.bfloat16), tokens_first(grads[1]).astype(jnp.bfloat16), tokens_first(grads[2]).astype(jnp.bfloat16), tokens_first(grads[3]).astype(jnp.float32))
```

```python
import jax
import jax.numpy as jnp
from jax import lax
from jax.experimental import pallas as pl
from jax.experimental.pallas import tpu as pltpu
from jax.sharding import Mesh
from jax.sharding import PartitionSpec as P

MESH = pl.DeviceIdType.MESH
SP = ("sp_0", "sp_1", "sp_2")
BF16 = jnp.bfloat16
F32 = jnp.float32
NY = 4
BLOCK = 64
VMEM = pl.BlockSpec(memory_space=pltpu.VMEM)
ANY = pl.BlockSpec(memory_space=pl.ANY)


def sizes():
    return lax.axis_size("sp_0"), lax.axis_size("sp_1")


def params(collective_id=None):
    if collective_id is None:
        return pltpu.CompilerParams(vmem_limit_bytes=60 * 1024 * 1024)
    return pltpu.CompilerParams(
        collective_id=collective_id, has_side_effects=True, vmem_limit_bytes=60 * 1024 * 1024
    )


def dot(a, b, ca, cb):
    return lax.dot_general(a, b, (((ca,), (cb,)), ((), ())), preferred_element_type=F32)


def place():
    return (
        lax.axis_index("sp_0"),
        lax.axis_index("sp_1"),
        lax.axis_index("sp_2"),
        lax.axis_index("tp"),
    )


def target(nx, zz, row, y):
    return (zz, row // 2, row % 2, y)


def offset(k):
    return jnp.where(k % 2 == 1, (k + 1) // 2, -(k // 2))


def settle(ref, sem):
    pltpu.make_async_copy(ref, ref, sem).wait()


def greet_plane(nz, nx, z, row, y, sides):
    barrier = pltpu.get_barrier_semaphore()
    rows = 2 * nx
    me = z * rows + row

    def hello(i, carry):
        peer = lax.rem(me + i, nz * rows)
        pl.semaphore_signal(
            barrier,
            inc=1,
            device_id=target(nx, peer // rows, lax.rem(peer, rows), y),
            device_id_type=MESH,
        )
        return carry

    lax.fori_loop(1, nz * rows, hello, 0)
    count = nz * rows - 1
    if sides:
        for side in (1, NY - 1):
            pl.semaphore_signal(
                barrier,
                inc=1,
                device_id=target(nx, z, row, lax.rem(y + side, NY)),
                device_id_type=MESH,
            )
        count += 2
    pl.semaphore_wait(barrier, count)


def remote(src, dst, send_sem, recv_sem, device):
    copy = pltpu.make_async_remote_copy(
        src_ref=src,
        dst_ref=dst,
        send_sem=send_sem,
        recv_sem=recv_sem,
        device_id=device,
        device_id_type=MESH,
    )
    copy.start()


def route_kernel(ids_ref, weights_ref, moe_ref, cot_ref, send_ref, pick_ref, own_ref, moe_q, cot_q, sem):
    tok, quarter = moe_q.shape
    slots = 2 * tok
    y = lax.axis_index("tp")
    cols = pl.ds(pl.multiple_of(y * quarter, quarter), quarter)
    first = pltpu.make_async_copy(moe_ref.at[:, cols], moe_q, sem.at[0])
    second = pltpu.make_async_copy(cot_ref.at[:, cols], cot_q, sem.at[1])
    first.start()
    second.start()
    experts = send_ref.shape[0]
    per = slots // experts
    lanes = max(128, experts)
    which = lax.broadcasted_iota(jnp.int32, (tok, lanes), 1)
    hot = [(ids_ref[:, j : j + 1] == which).astype(F32) for j in range(2)]
    lower = (
        lax.broadcasted_iota(jnp.int32, (tok, tok), 1)
        < lax.broadcasted_iota(jnp.int32, (tok, tok), 0)
    ).astype(BF16)
    before = dot(lower, (hot[0] + hot[1]).astype(BF16), 1, 0)
    slot_iota = lax.broadcasted_iota(jnp.int32, (tok, slots), 1)
    picks = []
    for j in range(2):
        rank = jnp.sum(before * hot[j], axis=1, keepdims=True).astype(jnp.int32)
        slot = ids_ref[:, j : j + 1] * per + rank
        picks.append((slot == slot_iota).astype(BF16))
    both = picks[0] + picks[1]
    pick_ref[...] = both
    first.wait()
    rows = dot(both, moe_q[...], 0, 0).astype(BF16)
    send_ref[:, :, 0:quarter] = rows.reshape(experts, per, quarter)
    second.wait()
    cot = cot_q[...]
    own_ref[...] = cot
    cot32 = cot.astype(F32)
    total = jnp.zeros((slots, quarter), F32)
    for j in range(2):
        scaled = (weights_ref[:, j : j + 1] * cot32).astype(BF16)
        total = total + dot(picks[j], scaled, 0, 0)
    send_ref[:, :, quarter:] = total.astype(BF16).reshape(experts, per, quarter)


def route(ids, weights, moe, cot):
    nz, nx = sizes()
    experts = nz * nx * 2
    tok, width = moe.shape
    quarter = width // NY
    per = 2 * tok // experts
    return pl.pallas_call(
        route_kernel,
        name="route",
        out_shape=(
            jax.ShapeDtypeStruct((experts, per, 2 * quarter), BF16),
            jax.ShapeDtypeStruct((tok, 2 * tok), BF16),
            jax.ShapeDtypeStruct((tok, quarter), BF16),
        ),
        in_specs=[VMEM, VMEM, ANY, ANY],
        out_specs=(VMEM, VMEM, VMEM),
        scratch_shapes=[
            pltpu.VMEM((tok, quarter), BF16),
            pltpu.VMEM((tok, quarter), BF16),
            pltpu.SemaphoreType.DMA((2,)),
        ],
        compiler_params=params(),
    )(ids, weights, moe, cot)


def dispatch_kernel(nz, nx, send_ref, out_ref, own_sem, send_sem, ring_sem, come, from_l, from_r, far_l, far_r):
    z, x, c, y = place()
    rows = 2 * nx
    row = x * 2 + c
    me = z * rows + row
    half = rows // 2
    right = target(nx, z, row, lax.rem(y + 1, NY))
    left = target(nx, z, row, lax.rem(y + NY - 1, NY))
    y_left, y_right = lax.rem(y + NY - 1, NY), lax.rem(y + 1, NY)
    greet_plane(nz, nx, z, row, y, True)
    own = pltpu.make_async_copy(send_ref.at[me], out_ref.at[y, me], own_sem)
    own.start()

    def scatter(i, carry):
        k, j = i // rows, lax.rem(i, rows)
        zz = lax.rem(z - offset(k) + nz, nz)
        to = lax.rem(row + j, rows)
        remote(
            send_ref.at[zz * rows + to],
            out_ref.at[y, me],
            send_sem,
            come.at[k],
            target(nx, zz, to, y),
        )
        return carry

    lax.fori_loop(1, nz * rows, scatter, 0)
    own.wait()

    def spread(k):
        part = pl.ds(lax.rem(z + offset(k) + nz, nz) * rows, rows)
        block = out_ref.at[y, part]
        remote(block, block, ring_sem, from_l.at[k], right)
        remote(block, block, ring_sem, from_r.at[k], left)

    def onward(k):
        at = lax.rem(z + offset(k) + nz, nz) * rows
        settle(out_ref.at[y_left, pl.ds(at, rows)], from_l.at[k])
        block = out_ref.at[y_left, pl.ds(at, half)]
        remote(block, block, ring_sem, far_l.at[k], right)
        settle(out_ref.at[y_right, pl.ds(at, rows)], from_r.at[k])
        block = out_ref.at[y_right, pl.ds(at + half, half)]
        remote(block, block, ring_sem, far_r.at[k], left)

    settle(out_ref.at[y, pl.ds(0, rows - 1)], come.at[0])
    spread(0)

    def step(k, carry):
        settle(out_ref.at[y, pl.ds(0, rows)], come.at[k])
        spread(k)
        onward(k - 1)
        return carry

    lax.fori_loop(1, nz, step, 0)
    onward(nz - 1)

    def finish(k, carry):
        settle(out_ref.at[y, pl.ds(0, half)], far_l.at[k])
        settle(out_ref.at[y, pl.ds(0, half)], far_r.at[k])
        return carry

    lax.fori_loop(0, nz, finish, 0)
    settle(send_ref.at[pl.ds(0, nz * rows - 1)], send_sem)
    settle(out_ref.at[pl.ds(0, 3)], ring_sem)


def dispatch(send):
    nz, nx = sizes()
    experts, per, width = send.shape

    def body(*refs):
        dispatch_kernel(nz, nx, *refs)

    return pl.pallas_call(
        body,
        name="dispatch",
        out_shape=jax.ShapeDtypeStruct((NY, experts, per, width), BF16),
        in_specs=[VMEM],
        out_specs=VMEM,
        scratch_shapes=[pltpu.SemaphoreType.DMA] * 3 + [pltpu.SemaphoreType.DMA((nz,))] * 5,
        compiler_params=params(1),
    )(send)


def expert_kernel(rows_ref, gate_ref, up_ref, down_ref, g_gate, g_up, g_down, part_ref):
    quarter = part_ref.shape[2]
    slots, units = rows_ref.shape[1], gate_ref.shape[1]
    pre_gate = jnp.zeros((slots, units), F32)
    pre_up = jnp.zeros((slots, units), F32)
    delta = jnp.zeros((slots, units), F32)
    for q in range(NY):
        cols = slice(q * quarter, (q + 1) * quarter)
        routed = rows_ref[q, :, 0:quarter]
        pre_gate = pre_gate + dot(routed, gate_ref[cols, :], 1, 0)
        pre_up = pre_up + dot(routed, up_ref[cols, :], 1, 0)
        delta = delta + dot(rows_ref[q, :, quarter:], down_ref[:, cols], 1, 1)
    sig = jax.nn.sigmoid(pre_gate)
    act = pre_gate * sig
    hidden = (act * pre_up).astype(BF16)
    d_gate = (delta * pre_up * sig * (1.0 + pre_gate * (1.0 - sig))).astype(BF16)
    d_up = (delta * act).astype(BF16)
    for q in range(NY):
        cols = slice(q * quarter, (q + 1) * quarter)
        part = dot(d_gate, gate_ref[cols, :], 1, 1) + dot(d_up, up_ref[cols, :], 1, 1)
        part_ref[q] = part.astype(BF16)
    for q in range(NY):
        cols = slice(q * quarter, (q + 1) * quarter)
        routed = rows_ref[q, :, 0:quarter]
        g_gate[cols, :] = dot(routed, d_gate, 0, 0).astype(BF16)
        g_up[cols, :] = dot(routed, d_up, 0, 0).astype(BF16)
        g_down[:, cols] = dot(hidden, rows_ref[q, :, quarter:], 0, 0).astype(BF16)


def expert(rows, gate, up, down):
    _, slots, width = rows.shape
    return pl.pallas_call(
        expert_kernel,
        name="expert",
        out_shape=(
            jax.ShapeDtypeStruct(gate.shape, BF16),
            jax.ShapeDtypeStruct(up.shape, BF16),
            jax.ShapeDtypeStruct(down.shape, BF16),
            jax.ShapeDtypeStruct((NY, slots, width // 2), BF16),
        ),
        in_specs=[VMEM] * 4,
        out_specs=(VMEM,) * 4,
        compiler_params=params(),
    )(rows, gate, up, down)


def giveback_kernel(
    nz, nx, part_ref, out_ref, near_l, near_r, sum_l, sum_r, last_l, last_r, done,
    own_sem, home_sem, ring_sem, ret_sem, a_l, a_r, b_l, b_r,
):
    z, x, c, y = place()
    rows = 2 * nx
    row = x * 2 + c
    me = z * rows + row
    half = rows // 2
    y_left, y_right = lax.rem(y + NY - 1, NY), lax.rem(y + 1, NY)
    y_far = lax.rem(y + 2, NY)
    right = target(nx, z, row, y_right)
    left = target(nx, z, row, y_left)
    greet_plane(nz, nx, z, row, y, True)

    def start_of(k):
        return lax.rem(z + offset(nz - 1 - k) + nz, nz) * rows

    def first(k, carry):
        at = start_of(k)
        remote(part_ref.at[y_far, pl.ds(at, half)], near_l.at[k], ring_sem, a_l.at[k], right)
        remote(part_ref.at[y_far, pl.ds(at + half, half)], near_r.at[k], ring_sem, a_r.at[k], left)
        return carry

    lax.fori_loop(0, nz, first, 0)

    def second(k):
        at = start_of(k)
        remote(
            part_ref.at[y_right, pl.ds(at + half, half)],
            last_l.at[k, pl.ds(half, half)], ring_sem, b_l.at[k], right,
        )
        remote(
            part_ref.at[y_left, pl.ds(at, half)],
            last_r.at[k, pl.ds(0, half)], ring_sem, b_r.at[k], left,
        )
        settle(near_l.at[k], a_l.at[k])
        sum_r[k] = (
            part_ref[y_right, pl.ds(at, half)].astype(F32) + near_l[k].astype(F32)
        ).astype(BF16)
        remote(sum_r.at[k], last_l.at[k, pl.ds(0, half)], ring_sem, b_l.at[k], right)
        settle(near_r.at[k], a_r.at[k])
        sum_l[k] = (
            part_ref[y_left, pl.ds(at + half, half)].astype(F32) + near_r[k].astype(F32)
        ).astype(BF16)
        remote(sum_l.at[k], last_r.at[k, pl.ds(half, half)], ring_sem, b_r.at[k], left)

    def third(k):
        at = start_of(k)
        settle(last_l.at[k], b_l.at[k])
        settle(last_r.at[k], b_r.at[k])
        done[k] = (
            part_ref[y, pl.ds(at, rows)].astype(F32)
            + last_l[k].astype(F32)
            + last_r[k].astype(F32)
        ).astype(BF16)

    def home(k, j):
        zz = lax.rem(z + offset(nz - 1 - k) + nz, nz)
        to = lax.rem(row + j, rows)
        remote(done.at[k, to], out_ref.at[me], home_sem, ret_sem, target(nx, zz, to, y))

    second(0)

    def step(k, carry):
        second(k)
        third(k - 1)

        def one(j, inner):
            home(k - 1, j)
            return inner

        lax.fori_loop(0, rows, one, 0)
        return carry

    lax.fori_loop(1, nz, step, 0)
    third(nz - 1)

    def one_last(j, inner):
        home(nz - 1, j)
        return inner

    lax.fori_loop(1, rows, one_last, 0)
    own = pltpu.make_async_copy(done.at[nz - 1, row], out_ref.at[me], own_sem)
    own.start()
    own.wait()
    settle(out_ref.at[pl.ds(0, nz * rows - 1)], ret_sem)
    settle(out_ref.at[pl.ds(0, nz * rows - 1)], home_sem)
    settle(part_ref.at[pl.ds(0, 3)], ring_sem)


def giveback(part):
    nz, nx = sizes()
    _, experts, per, quarter = part.shape
    rows = 2 * nx
    half = rows // 2

    def body(*refs):
        giveback_kernel(nz, nx, *refs)

    return pl.pallas_call(
        body,
        name="giveback",
        out_shape=jax.ShapeDtypeStruct((experts, per, quarter), BF16),
        in_specs=[VMEM],
        out_specs=VMEM,
        scratch_shapes=[pltpu.VMEM((nz, half, per, quarter), BF16)] * 4
        + [pltpu.VMEM((nz, rows, per, quarter), BF16)] * 3
        + [pltpu.SemaphoreType.DMA] * 4
        + [pltpu.SemaphoreType.DMA((nz,))] * 4,
        compiler_params=params(2),
    )(part)


def collect_kernel(nx, pick_ref, ret_ref, own_ref, out_ref, ring_sem, from_l, from_r, far_l, far_r):
    z, x, c, y = place()
    row = x * 2 + c
    pieces, span = out_ref.shape[1], out_ref.shape[2]
    half = span // 2
    y_left, y_right = lax.rem(y + NY - 1, NY), lax.rem(y + 1, NY)
    right = target(nx, z, row, y_right)
    left = target(nx, z, row, y_left)
    barrier = pltpu.get_barrier_semaphore()
    pl.semaphore_signal(barrier, inc=1, device_id=left, device_id_type=MESH)
    pl.semaphore_signal(barrier, inc=1, device_id=right, device_id_type=MESH)
    pl.semaphore_wait(barrier, 2)
    for i in range(pieces):
        lines = slice(i * span, (i + 1) * span)
        both = dot(pick_ref[lines, :], ret_ref[...], 1, 0)
        out_ref[y, i] = (own_ref[lines, :].astype(F32) + both).astype(BF16)
        block = out_ref.at[y, i]
        remote(block, block, ring_sem, from_l.at[i], right)
        remote(block, block, ring_sem, from_r.at[i], left)

    def onward(i, carry):
        settle(out_ref.at[y_left, i], from_l.at[i])
        block = out_ref.at[y_left, i, pl.ds(0, half)]
        remote(block, block, ring_sem, far_l.at[i], right)
        settle(out_ref.at[y_right, i], from_r.at[i])
        block = out_ref.at[y_right, i, pl.ds(half, half)]
        remote(block, block, ring_sem, far_r.at[i], left)
        return carry

    lax.fori_loop(0, pieces, onward, 0)

    def finish(i, carry):
        settle(out_ref.at[y, i, pl.ds(0, half)], far_l.at[i])
        settle(out_ref.at[y, i, pl.ds(0, half)], far_r.at[i])
        return carry

    lax.fori_loop(0, pieces, finish, 0)
    settle(out_ref.at[pl.ds(0, 3)], ring_sem)


def collect(pick, returned, own):
    _, nx = sizes()
    tok, quarter = own.shape
    pieces = 4

    def body(*refs):
        collect_kernel(nx, *refs)

    return pl.pallas_call(
        body,
        name="collect",
        out_shape=jax.ShapeDtypeStruct((NY, pieces, tok // pieces, quarter), BF16),
        in_specs=[VMEM] * 3,
        out_specs=VMEM,
        scratch_shapes=[pltpu.SemaphoreType.DMA] + [pltpu.SemaphoreType.DMA((pieces,))] * 4,
        compiler_params=params(3),
    )(pick, returned, own)


def triangle(kind):
    row = lax.broadcasted_iota(jnp.int32, (BLOCK, BLOCK), 0)
    col = lax.broadcasted_iota(jnp.int32, (BLOCK, BLOCK), 1)
    return {"le": col <= row, "ge": col >= row, "lt": col < row}[kind]


def spread_sum(tri, value):
    high = value.astype(BF16)
    rest = value - high.astype(F32)
    mid = rest.astype(BF16)
    low = (rest - mid.astype(F32)).astype(BF16)
    both = jnp.concatenate([high, mid, low], axis=0)
    return dot(jnp.concatenate([tri, tri, tri], axis=1), both, 1, 0)


def diagonal(shape):
    return (lax.broadcasted_iota(jnp.int32, shape, 0) < shape[0] // 2) == (
        lax.broadcasted_iota(jnp.int32, shape, 1) < shape[1] // 2
    )


def local_kernel(
    tg_ref, ow_ref, mix_ref, q_ref, k_ref, v_ref, ld_ref, cot_ref, gw_ref, pay_ref, cum_ref
):
    tok = q_ref.shape[0]
    quarter = tg_ref.shape[2]
    total = jnp.zeros((tok, ow_ref.shape[1]), F32)
    for q in range(NY):
        total = total + dot(tg_ref[q], ow_ref[q * quarter : (q + 1) * quarter, :], 1, 0)
    cot_ref[...] = total.astype(BF16)
    lines = gw_ref.shape[3]
    nz, nx = gw_ref.shape[2], gw_ref.shape[1]
    mix = mix_ref[...]
    for q in range(NY):
        grad = dot(tg_ref[q], mix, 0, 0).astype(BF16)
        for m in range(quarter // lines):
            sp = q * (quarter // lines) + m
            gw_ref[sp % 2, (sp // 2) % nx, sp // (2 * nx)] = grad[m * lines : (m + 1) * lines, :]
    tri = triangle("le").astype(BF16)
    blocks = tok // BLOCK
    same = diagonal((2 * 128, 128))
    state = jnp.zeros((256, 128), F32)
    ends = []
    for b in range(blocks):
        at = slice(b * BLOCK, (b + 1) * BLOCK)
        cum = spread_sum(tri, ld_ref[at, :])
        cum_ref[at, :] = cum
        end = cum[BLOCK - 1 : BLOCK, :]
        ends.append(end)
        kept = (k_ref[at, :].astype(F32) * jnp.exp(end - cum)).astype(BF16)
        state = state * jnp.exp(end) + dot(v_ref[at, :], kept, 0, 0)
    pull = jnp.zeros((256, 128), F32)
    for b in reversed(range(blocks)):
        at = slice(b * BLOCK, (b + 1) * BLOCK)
        asked = (q_ref[at, :].astype(F32) * 0.125 * jnp.exp(cum_ref[at, :])).astype(BF16)
        pull = pull * jnp.exp(ends[b]) + dot(cot_ref[at, :], asked, 0, 0)
    state = jnp.where(same, state, 0.0)
    pull = jnp.where(same, pull, 0.0)
    state = state[0:128] + state[128:256]
    pull = pull[0:128] + pull[128:256]
    whole = ends[0]
    for b in range(1, blocks):
        whole = whole + ends[b]
    rows = pay_ref.shape[0]
    span = 128 // rows
    for i in range(rows):
        pay_ref[i, 0:span, :] = state[i * span : (i + 1) * span]
        pay_ref[i, span : 2 * span, :] = pull[i * span : (i + 1) * span]
        pay_ref[i, 2 * span :, :] = jnp.broadcast_to(whole, (8, 128))


def local_part(token_grad, out_weight, mixer_out, query, key, value, log_decay):
    nz, nx = sizes()
    rows = 2 * nx
    tok = query.shape[0]
    lines = out_weight.shape[0] // (nz * rows)
    return pl.pallas_call(
        local_kernel,
        name="local",
        out_shape=(
            jax.ShapeDtypeStruct((tok, 256), BF16),
            jax.ShapeDtypeStruct((2, nx, nz, lines, 256), BF16),
            jax.ShapeDtypeStruct((rows, 2 * (128 // rows) + 8, 128), F32),
            jax.ShapeDtypeStruct((tok, 128), F32),
        ),
        in_specs=[VMEM] * 7,
        out_specs=(VMEM,) * 4,
        compiler_params=params(),
    )(token_grad, out_weight, mixer_out, query, key, value, log_decay)


def exchange_kernel(
    nz, nx, pay_ref, gw_ref, ex_ref, gout_ref,
    row_in, z_out, z_in, row_out, core_in, x_out, x_in, last_out, last_in, ends,
    own_sem, sent, p1, p2, p3, g1, g2, g3,
):
    z, x, c, y = place()
    rows = 2 * nx
    row = x * 2 + c
    span = 128 // rows
    barrier = pltpu.get_barrier_semaphore()

    def greet_row(j, carry):
        pl.semaphore_signal(
            barrier, inc=1, device_id=target(nx, z, lax.rem(row + j, rows), y), device_id_type=MESH
        )
        return carry

    def greet_z(j, carry):
        pl.semaphore_signal(
            barrier, inc=1, device_id=target(nx, lax.rem(z + j, nz), row, y), device_id_type=MESH
        )
        return carry

    lax.fori_loop(1, rows, greet_row, 0)
    lax.fori_loop(1, nz, greet_z, 0)
    pl.semaphore_wait(barrier, rows + nz - 2)

    def row_send(j, carry):
        to = lax.rem(row + j, rows)
        remote(pay_ref.at[to], row_in.at[row], sent.at[0], p1, target(nx, z, to, y))
        return carry

    lax.fori_loop(1, rows, row_send, 0)
    remote(gw_ref.at[1 - c], core_in, sent.at[3], g1, (z, x, 1 - c, y))
    own = pltpu.make_async_copy(pay_ref.at[row], row_in.at[row], own_sem)
    own.start()
    own.wait()

    settle(row_in.at[pl.ds(0, rows - 1)], p1)
    state = jnp.zeros((span, 128), F32)
    after = jnp.zeros((1, 128), F32)
    for j in range(rows):
        row_out[j, 0:span, :] = state
        ends[j : j + 1, :] = after
        keep = row_in[j, 2 * span : 2 * span + 1, :]
        state = state * jnp.exp(keep) + row_in[j, 0:span, :]
        after = after + keep
    pull = jnp.zeros((span, 128), F32)
    for j in reversed(range(rows)):
        row_out[j, span : 2 * span, :] = pull
        pull = pull * jnp.exp(row_in[j, 2 * span : 2 * span + 1, :]) + row_in[j, span : 2 * span, :]
    z_out[0:span, :] = state
    z_out[span : 2 * span, :] = pull
    z_out[2 * span :, :] = jnp.broadcast_to(after, (8, 128))
    z_in[z] = z_out[...]

    def z_send(j, carry):
        remote(z_out, z_in.at[z], sent.at[1], p2, target(nx, lax.rem(z + j, nz), row, y))
        return carry

    lax.fori_loop(1, nz, z_send, 0)

    settle(core_in, g1)
    for xx in range(nx):
        x_out[xx] = (gw_ref[c, xx].astype(F32) + core_in[xx].astype(F32)).astype(BF16)

    def x_send(j, carry):
        to = lax.rem(x + j, nx)
        remote(x_out.at[to], x_in.at[x], sent.at[4], g2, (z, to, c, y))
        return carry

    lax.fori_loop(1, nx, x_send, 0)

    settle(z_in.at[pl.ds(0, nz - 1)], p2)
    state = jnp.zeros((span, 128), F32)
    mine = jnp.zeros((span, 128), F32)
    for k in range(nz):
        mine = jnp.where(z == k, state, mine)
        state = state * jnp.exp(z_in[k, 2 * span : 2 * span + 1, :]) + z_in[k, 0:span, :]
    pull = jnp.zeros((span, 128), F32)
    mine_pull = jnp.zeros((span, 128), F32)
    for k in reversed(range(nz)):
        mine_pull = jnp.where(z == k, pull, mine_pull)
        pull = pull * jnp.exp(z_in[k, 2 * span : 2 * span + 1, :]) + z_in[k, span : 2 * span, :]
    behind = jnp.zeros((1, 128), F32)
    for j in reversed(range(rows)):
        row_out[j, 0:span, :] = row_out[j, 0:span, :] + mine * jnp.exp(ends[j : j + 1, :])
        row_out[j, span : 2 * span, :] = row_out[j, span : 2 * span, :] + mine_pull * jnp.exp(behind)
        behind = behind + row_in[j, 2 * span : 2 * span + 1, :]

    def row_back(j, carry):
        to = lax.rem(row + j, rows)
        remote(row_out.at[to], ex_ref.at[row], sent.at[2], p3, target(nx, z, to, y))
        return carry

    lax.fori_loop(1, rows, row_back, 0)
    ex_ref[row] = row_out[row]

    settle(x_in.at[pl.ds(0, nx - 1)], g2)
    total = x_out[x].astype(F32)
    for j in range(1, nx):
        total = total + x_in[lax.rem(x + j, nx)].astype(F32)
    last_out[...] = total.astype(BF16)

    def last_send(j, carry):
        to = lax.rem(z + j, nz)
        remote(last_out.at[to], last_in.at[z], sent.at[5], g3, (to, x, c, y))
        return carry

    lax.fori_loop(1, nz, last_send, 0)
    settle(last_in.at[pl.ds(0, nz - 1)], g3)
    total = last_out[z].astype(F32)
    for j in range(1, nz):
        total = total + last_in[lax.rem(z + j, nz)].astype(F32)
    gout_ref[...] = total

    settle(ex_ref.at[pl.ds(0, rows - 1)], p3)
    settle(pay_ref.at[pl.ds(0, rows - 1)], sent.at[0])
    settle(z_in.at[pl.ds(0, nz - 1)], sent.at[1])
    settle(ex_ref.at[pl.ds(0, rows - 1)], sent.at[2])
    settle(core_in, sent.at[3])
    settle(x_in.at[pl.ds(0, nx - 1)], sent.at[4])
    settle(last_in.at[pl.ds(0, nz - 1)], sent.at[5])


def exchange(pay, gw):
    nz, nx = sizes()
    rows, deep, _ = pay.shape
    lines = gw.shape[3]
    span = 128 // rows

    def body(*refs):
        exchange_kernel(nz, nx, *refs)

    return pl.pallas_call(
        body,
        name="exchange",
        out_shape=(
            jax.ShapeDtypeStruct((rows, 2 * span, 128), F32),
            jax.ShapeDtypeStruct((lines, 256), F32),
        ),
        in_specs=[VMEM, VMEM],
        out_specs=(VMEM, VMEM),
        scratch_shapes=[
            pltpu.VMEM((rows, deep, 128), F32),
            pltpu.VMEM((deep, 128), F32),
            pltpu.VMEM((nz, deep, 128), F32),
            pltpu.VMEM((rows, 2 * span, 128), F32),
            pltpu.VMEM((nx, nz, lines, 256), BF16),
            pltpu.VMEM((nx, nz, lines, 256), BF16),
            pltpu.VMEM((nx, nz, lines, 256), BF16),
            pltpu.VMEM((nz, lines, 256), BF16),
            pltpu.VMEM((nz, lines, 256), BF16),
            pltpu.VMEM((rows, 128), F32),
        ]
        + [pltpu.SemaphoreType.DMA, pltpu.SemaphoreType.DMA((6,))]
        + [pltpu.SemaphoreType.DMA] * 6,
        compiler_params=params(4),
    )(pay, gw)


def attention_kernel(q_ref, k_ref, v_ref, cot_ref, cum_ref, ex_ref, dq_ref, dk_ref, dv_ref, dl_ref, states):
    tok = q_ref.shape[0]
    blocks = tok // BLOCK
    rows = ex_ref.shape[0]
    span = 128 // rows
    same = diagonal((256, 128))
    head0 = lax.broadcasted_iota(jnp.int32, (BLOCK, 128), 1) < 64
    le = triangle("le")
    ge = triangle("ge").astype(BF16)
    lt = triangle("lt").astype(BF16)

    def opened(lower):
        compact = jnp.concatenate([ex_ref[i, lower : lower + span, :] for i in range(rows)], axis=0)
        return jnp.where(same, jnp.concatenate([compact, compact], axis=0), 0.0)

    state = opened(0)
    for b in range(blocks):
        states[b] = state
        if b + 1 < blocks:
            at = slice(b * BLOCK, (b + 1) * BLOCK)
            cum = cum_ref[at, :]
            end = cum[BLOCK - 1 : BLOCK, :]
            kept = (k_ref[at, :].astype(F32) * jnp.exp(end - cum)).astype(BF16)
            state = state * jnp.exp(end) + jnp.where(same, dot(v_ref[at, :], kept, 0, 0), 0.0)
    pull = opened(span)
    for b in reversed(range(blocks)):
        at = slice(b * BLOCK, (b + 1) * BLOCK)
        cum = cum_ref[at, :]
        end = cum[BLOCK - 1 : BLOCK, :]
        middle = cum[BLOCK // 2 - 1 : BLOCK // 2, :]
        query = q_ref[at, :].astype(F32) * 0.125
        key = k_ref[at, :].astype(F32)
        up, down = jnp.exp(cum - middle), jnp.exp(middle - cum)
        q_mid = (query * up).astype(BF16)
        k_mid = (key * down).astype(BF16)
        asked_decay, kept_decay = jnp.exp(cum), jnp.exp(end - cum)
        asked = (query * asked_decay).astype(BF16)
        kept = (key * kept_decay).astype(BF16)
        nothing = jnp.zeros_like(q_mid)
        dq_mid = jnp.zeros((BLOCK, 128), F32)
        dk_mid = jnp.zeros((BLOCK, 128), F32)
        for h in range(2):
            cols = slice(h * 128, (h + 1) * 128)
            mine = head0 if h == 0 else jnp.logical_not(head0)
            q_one = jnp.where(mine, q_mid, nothing)
            k_one = jnp.where(mine, k_mid, nothing)
            cot = cot_ref[at, cols]
            scores = jnp.where(le, dot(q_one, k_one, 1, 1), 0.0).astype(BF16)
            d_scores = jnp.where(le, dot(cot, v_ref[at, cols], 1, 1), 0.0).astype(BF16)
            dq_mid = dq_mid + dot(d_scores, k_one, 1, 0)
            dk_mid = dk_mid + dot(d_scores, q_one, 0, 0)
            dv_ref[at, cols] = (
                dot(scores, cot, 0, 0) + dot(kept, pull[cols, :].astype(BF16), 1, 1)
            ).astype(BF16)
        state = states[b]
        cot = cot_ref[at, :]
        dq_far = dot(cot, state.astype(BF16), 1, 0)
        dk_far = dot(v_ref[at, :], pull.astype(BF16), 1, 0)
        dq_ref[at, :] = ((dq_mid * up + dq_far * asked_decay) * 0.125).astype(BF16)
        dk_ref[at, :] = (dk_mid * down + dk_far * kept_decay).astype(BF16)
        near = q_mid.astype(F32) * dq_mid - k_mid.astype(F32) * dk_mid
        near = near + query * asked_decay * dq_far
        far = key * kept_decay * dk_far
        carried = jnp.sum(state * pull, axis=0, keepdims=True) * jnp.exp(end)
        dl_ref[at, :] = spread_sum(ge, near) + spread_sum(lt, far) + carried
        if b:
            pull = pull * jnp.exp(end) + jnp.where(same, dot(cot, asked, 0, 0), 0.0)


def attention(query, key, value, cot, cum, ex):
    tok = query.shape[0]
    return pl.pallas_call(
        attention_kernel,
        name="attention",
        out_shape=(
            jax.ShapeDtypeStruct((tok, 128), BF16),
            jax.ShapeDtypeStruct((tok, 128), BF16),
            jax.ShapeDtypeStruct((tok, 256), BF16),
            jax.ShapeDtypeStruct((tok, 128), F32),
        ),
        in_specs=[VMEM] * 6,
        out_specs=(VMEM,) * 4,
        scratch_shapes=[pltpu.VMEM((tok // BLOCK, 256, 128), F32)],
        compiler_params=params(),
    )(query, key, value, cot, cum, ex)


def shards(
    moe_input,
    cotangent,
    expert_ids,
    route_weights,
    gate_weight,
    up_weight,
    down_weight,
    out_weight,
    mixer_out,
    query_vectors,
    key_vectors,
    value_vectors,
    log_decay,
):
    tok, width = moe_input.shape
    quarter = width // NY
    send, pick, own_cot = route(expert_ids, route_weights, moe_input, cotangent)
    experts, per, _ = send.shape
    gathered = dispatch(send).reshape(NY, experts * per, 2 * quarter)
    grad_gate, grad_up, grad_down, part = expert(
        gathered, gate_weight[0], up_weight[0], down_weight[0]
    )
    returned = giveback(part.reshape(NY, experts, per, quarter))
    token_grad = collect(pick, returned.reshape(experts * per, quarter), own_cot)
    cot, gw, pay, cum = local_part(
        token_grad.reshape(NY, tok, quarter),
        out_weight,
        mixer_out,
        query_vectors,
        key_vectors,
        value_vectors,
        log_decay,
    )
    ex, grad_out_weight = exchange(pay, gw)
    grads = attention(query_vectors, key_vectors, value_vectors, cot, cum, ex)
    return (
        grad_gate[None],
        grad_up[None],
        grad_down[None],
        grad_out_weight,
        grads[0],
        grads[1],
        grads[2],
        grads[3],
    )


def solution(mesh):
    finer = Mesh(mesh.devices.reshape(8, 4, 2, mesh.shape["tp"]), ("sp_0", "sp_1", "sp_2", "tp"))
    in_specs = (
        P(SP, None),
        P(SP, None),
        P(SP, None),
        P(SP, None),
        P(SP, None, "tp"),
        P(SP, None, "tp"),
        P(SP, "tp", None),
        P(None, "tp"),
        P(SP, "tp"),
        P(SP, "tp"),
        P(SP, "tp"),
        P(SP, "tp"),
        P(SP, "tp"),
    )
    out_specs = (
        P(SP, None, "tp"),
        P(SP, None, "tp"),
        P(SP, "tp", None),
        P(SP, "tp"),
        P(SP, "tp"),
        P(SP, "tp"),
        P(SP, "tp"),
        P(SP, "tp"),
    )
    return jax.shard_map(
        shards, mesh=finer, in_specs=in_specs, out_specs=out_specs, check_vma=False
    )
```

```python
import jax
import jax.numpy as jnp
from jax import lax
from jax.experimental import pallas as pl
from jax.experimental.pallas import tpu as pltpu
from jax.sharding import Mesh
from jax.sharding import PartitionSpec as P

MESH = pl.DeviceIdType.MESH
SP = ("sp_0", "sp_1", "sp_2")
BF16 = jnp.bfloat16
F32 = jnp.float32
NY = 4
TRAIL = 2
ORDER = {8: (0, 2, 6, 3, 5, 4, 1, 7)}
BLOCK = 64
VMEM = pl.BlockSpec(memory_space=pltpu.VMEM)
ANY = pl.BlockSpec(memory_space=pl.ANY)


def sizes():
    return lax.axis_size("sp_0"), lax.axis_size("sp_1")


def params(collective_id=None):
    if collective_id is None:
        return pltpu.CompilerParams(vmem_limit_bytes=60 * 1024 * 1024)
    return pltpu.CompilerParams(
        collective_id=collective_id, has_side_effects=True, vmem_limit_bytes=60 * 1024 * 1024
    )


def dot(a, b, ca, cb):
    return lax.dot_general(a, b, (((ca,), (cb,)), ((), ())), preferred_element_type=F32)


def place():
    return (
        lax.axis_index("sp_0"),
        lax.axis_index("sp_1"),
        lax.axis_index("sp_2"),
        lax.axis_index("tp"),
    )


def target(nx, zz, row, y):
    return (zz, row // 2, row % 2, y)


def offset(k, nz):
    order = ORDER.get(nz, tuple(range(nz)))
    out = 0
    for i, ahead in enumerate(order):
        out = out + jnp.where(k == i, ahead, 0)
    return out


def settle(ref, sem):
    pltpu.make_async_copy(ref, ref, sem).wait()


def greet_plane(barrier, nz, nx, z, row, y):
    rows = 2 * nx
    me = z * rows + row

    def hello(i, carry):
        far = jnp.where(i % 2 == 0, nz * rows // 2 - i // 2, nz * rows // 2 + 1 + i // 2)
        peer = lax.rem(me + far, nz * rows)
        pl.semaphore_signal(
            barrier,
            inc=1,
            device_id=target(nx, peer // rows, lax.rem(peer, rows), y),
            device_id_type=MESH,
        )
        return carry

    lax.fori_loop(0, nz * rows - 1, hello, 0)
    for side in (1, NY - 1):
        pl.semaphore_signal(
            barrier,
            inc=1,
            device_id=target(nx, z, row, lax.rem(y + side, NY)),
            device_id_type=MESH,
        )


def remote(src, dst, send_sem, recv_sem, device):
    copy = pltpu.make_async_remote_copy(
        src_ref=src,
        dst_ref=dst,
        send_sem=send_sem,
        recv_sem=recv_sem,
        device_id=device,
        device_id_type=MESH,
    )
    copy.start()


def triangle(kind):
    row = lax.broadcasted_iota(jnp.int32, (BLOCK, BLOCK), 0)
    col = lax.broadcasted_iota(jnp.int32, (BLOCK, BLOCK), 1)
    return {"le": col <= row, "ge": col >= row, "lt": col < row}[kind]


def spread_sum(tri, value):
    high = value.astype(BF16)
    rest = value - high.astype(F32)
    mid = rest.astype(BF16)
    low = (rest - mid.astype(F32)).astype(BF16)
    both = jnp.concatenate([high, mid, low], axis=0)
    return dot(jnp.concatenate([tri, tri, tri], axis=1), both, 1, 0)


def diagonal(shape):
    return (lax.broadcasted_iota(jnp.int32, shape, 0) < shape[0] // 2) == (
        lax.broadcasted_iota(jnp.int32, shape, 1) < shape[1] // 2
    )


def mega_kernel(r, nz, nx):
    z, x, c, y = place()
    rows = 2 * nx
    row = x * 2 + c
    me = z * rows + row
    half = rows // 2
    tok, quarter = r.moe_q.shape
    experts, per = nz * rows, 2 * tok // (nz * rows)
    slots = 2 * tok
    units = r.gate.shape[1]
    y_left, y_right = lax.rem(y + NY - 1, NY), lax.rem(y + 1, NY)
    y_far = lax.rem(y + 2, NY)
    right = target(nx, z, row, y_right)
    left = target(nx, z, row, y_left)
    cols = pl.ds(pl.multiple_of(y * quarter, quarter), quarter)
    loads = [
        pltpu.make_async_copy(src, dst, r.load_sem.at[i])
        for i, (src, dst) in enumerate(
            (
                (r.moe_hbm.at[:, cols], r.moe_q),
                (r.cot_hbm.at[:, cols], r.cot_q),
                (r.ld_hbm, r.ld),
                (r.k_hbm, r.k),
                (r.v_hbm, r.v),
                (r.gate_hbm, r.gate),
                (r.up_hbm, r.up),
                (r.down_hbm, r.down),
                (r.q_hbm, r.q),
                (r.ow_hbm, r.ow),
                (r.mix_hbm, r.mix),
                (r.moe_hbm, r.moe),
                (r.cot_hbm, r.cot),
            )
        )
    ]
    for load in loads:
        load.start()
    barrier = pltpu.get_barrier_semaphore()
    greet_plane(barrier, nz, nx, z, row, y)

    lanes = max(128, experts)
    which = lax.broadcasted_iota(jnp.int32, (lanes, tok), 0)
    hot = [(r.ids[j : j + 1, :] == which).astype(F32) for j in range(2)]
    earlier = (
        lax.broadcasted_iota(jnp.int32, (tok, tok), 0)
        < lax.broadcasted_iota(jnp.int32, (tok, tok), 1)
    ).astype(BF16)
    before = dot((hot[0] + hot[1]).astype(BF16), earlier, 1, 0)
    slot_iota = lax.broadcasted_iota(jnp.int32, (slots, tok), 0)
    picks = []
    for j in range(2):
        rank = jnp.sum(before * hot[j], axis=0, keepdims=True).astype(jnp.int32)
        slot = r.ids[j : j + 1, :] * per + rank
        picks.append((slot == slot_iota).astype(BF16))
    both = picks[0] + picks[1]
    r.pick[...] = both
    slot_weight = jnp.zeros((slots, 1), F32)
    for j in range(2):
        chosen = picks[j].astype(F32) * r.weights[j : j + 1, :]
        slot_weight = slot_weight + jnp.sum(chosen, axis=1, keepdims=True)
    r.slot_weight[...] = jnp.broadcast_to(slot_weight, (slots, 128))
    loads[0].wait()
    sorted_rows = dot(both, r.moe_q[...], 1, 0).astype(BF16)
    r.send[:, :, 0:quarter] = sorted_rows.reshape(experts, per, quarter)
    loads[1].wait()
    sorted_cot = (dot(both, r.cot_q[...], 1, 0) * slot_weight).astype(BF16)
    r.send[:, :, quarter:] = sorted_cot.reshape(experts, per, quarter)
    pl.semaphore_wait(barrier, nz * rows + 1)

    def scatter(i, carry):
        k, j = i // rows, lax.rem(i, rows)
        zz = lax.rem(z - offset(k, nz) + nz, nz)
        to = lax.rem(row + j, rows)
        remote(
            r.send.at[zz * rows + to],
            r.rows.at[y, k * rows + row],
            r.send_sem,
            r.come.at[k],
            target(nx, zz, to, y),
        )
        return carry

    ring = nz - 1 - TRAIL
    lax.fori_loop(rows, (ring + 1) * rows, scatter, 0)
    lines = rows * per
    loads[11].wait()
    loads[12].wait()
    for i, k in enumerate([0, *range(ring + 1, nz)]):
        zz = lax.rem(z - offset(k, nz) + nz, nz)
        there = pl.ds(pl.multiple_of(zz * lines, lines), lines)
        pick_there = r.pick[there, :]
        weight_there = r.slot_weight[there, 0:1]
        block = slice(i * rows, (i + 1) * rows)
        for q in range(NY):
            part = slice(q * quarter, (q + 1) * quarter)
            value = dot(pick_there, r.moe[:, part], 1, 0).astype(BF16)
            r.full[block, q, :, 0:quarter] = value.reshape(rows, per, quarter)
            value = (dot(pick_there, r.cot[:, part], 1, 0) * weight_there).astype(BF16)
            r.full[block, q, :, quarter:] = value.reshape(rows, per, quarter)

        def scatter_full(j, carry, i=i, k=k, zz=zz):
            to = lax.rem(row + j, rows)
            remote(
                r.full.at[i * rows + to],
                r.rows.at[:, k * rows + row],
                r.full_sem,
                r.come.at[k],
                target(nx, zz, to, y),
            )
            return carry

        lax.fori_loop(0 if i else 1, rows, scatter_full, 0)
    own = pltpu.make_async_copy(r.full.at[row], r.rows.at[:, row], r.own_sem.at[0])
    own.start()
    own.wait()

    blocks = tok // BLOCK
    same = diagonal((256, 128))
    tri = triangle("le").astype(BF16)
    for load in loads[2:5]:
        load.wait()
    state = jnp.zeros((256, 128), F32)
    for b in range(blocks):
        at = slice(b * BLOCK, (b + 1) * BLOCK)
        cum = spread_sum(tri, r.ld[at, :])
        r.cum[at, :] = cum
        end = cum[BLOCK - 1 : BLOCK, :]
        kept = (r.k[at, :].astype(F32) * jnp.exp(end - cum)).astype(BF16)
        added = jnp.where(same, dot(r.v[at, :], kept, 0, 0), 0.0)
        r.added[b] = added
        state = state * jnp.exp(end) + added
        whole = end if b == 0 else whole + end
    state = state[0:128] + state[128:256]
    span = 128 // rows
    for i in range(rows):
        r.f_pay[i, 0:span, :] = state[i * span : (i + 1) * span]
        r.f_pay[i, span:, :] = jnp.broadcast_to(whole, (8, 128))

    def f_send(j, carry):
        to = lax.rem(row + j, rows)
        remote(r.f_pay.at[to], r.f_row_in.at[row], r.f_sent.at[0], r.f1, target(nx, z, to, y))
        return carry

    lax.fori_loop(1, rows, f_send, 0)
    r.f_row_in[row] = r.f_pay[row]

    def kept_row(j):
        return r.f_row_in[j, span : span + 1, :]

    def kept_z(k):
        return r.f_z_in[k, span : span + 1, :]

    def forward_row():
        settle(r.f_row_in.at[pl.ds(0, rows - 1)], r.f1)
        state = jnp.zeros((span, 128), F32)
        after = jnp.zeros((1, 128), F32)
        for j in range(rows):
            r.f_row_out[j] = state
            r.ends[j : j + 1, :] = after
            state = state * jnp.exp(kept_row(j)) + r.f_row_in[j, 0:span, :]
            after = after + kept_row(j)
        r.f_z_out[0:span, :] = state
        r.f_z_out[span:, :] = jnp.broadcast_to(after, (8, 128))
        r.f_z_in[z] = r.f_z_out[...]

        def send(j, carry):
            to = lax.rem(z + j, nz)
            remote(r.f_z_out, r.f_z_in.at[z], r.f_sent.at[1], r.f2, target(nx, to, row, y))
            return carry

        lax.fori_loop(1, nz, send, 0)

    def forward_z():
        settle(r.f_z_in.at[pl.ds(0, nz - 1)], r.f2)
        state = jnp.zeros((span, 128), F32)
        mine = jnp.zeros((span, 128), F32)
        for k in range(nz):
            mine = jnp.where(z == k, state, mine)
            state = state * jnp.exp(kept_z(k)) + r.f_z_in[k, 0:span, :]
        for j in range(rows):
            r.f_row_out[j] = r.f_row_out[j] + mine * jnp.exp(r.ends[j : j + 1, :])

        def send(j, carry):
            to = lax.rem(row + j, rows)
            remote(r.f_row_out.at[to], r.f_ex.at[row], r.f_sent.at[2], r.f3, target(nx, z, to, y))
            return carry

        lax.fori_loop(1, rows, send, 0)
        r.f_ex[row] = r.f_row_out[row]

    for load in loads[5:11]:
        load.wait()

    def chunk(k):
        return pl.ds(k * rows, rows)

    def spread(k):
        block = r.rows.at[y, chunk(k)]
        remote(block, block, r.ring_sem, r.from_l.at[k], right)
        remote(block, block, r.ring_sem, r.from_r.at[k], left)

    def onward(k):
        settle(r.rows.at[y_left, chunk(k)], r.from_l.at[k])
        block = r.rows.at[y_left, pl.ds(k * rows, half)]
        remote(block, block, r.ring_sem, r.far_l.at[k], right)
        settle(r.rows.at[y_right, chunk(k)], r.from_r.at[k])
        block = r.rows.at[y_right, pl.ds(k * rows + half, half)]
        remote(block, block, r.ring_sem, r.far_r.at[k], left)

    def gathered(k):
        settle(r.rows.at[y, pl.ds(0, half)], r.far_l.at[k])
        settle(r.rows.at[y, pl.ds(0, half)], r.far_r.at[k])

    def expert(k):
        pre_gate = jnp.zeros((lines, units), F32)
        pre_up = jnp.zeros((lines, units), F32)
        delta = jnp.zeros((lines, units), F32)
        for q in range(NY):
            part = slice(q * quarter, (q + 1) * quarter)
            routed = r.rows[q, chunk(k), :, 0:quarter].reshape(lines, quarter)
            routed_cot = r.rows[q, chunk(k), :, quarter:].reshape(lines, quarter)
            pre_gate = pre_gate + dot(routed, r.gate[part, :], 1, 0)
            pre_up = pre_up + dot(routed, r.up[part, :], 1, 0)
            delta = delta + dot(routed_cot, r.down[:, part], 1, 1)
        sig = jax.nn.sigmoid(pre_gate)
        act = pre_gate * sig
        d_gate = (delta * pre_up * sig * (1.0 + pre_gate * (1.0 - sig))).astype(BF16)
        d_up = (delta * act).astype(BF16)
        at = pl.ds(pl.multiple_of(k * lines, lines), lines)
        r.hidden[at, :] = (act * pre_up).astype(BF16)
        r.d_gate[at, :] = d_gate
        r.d_up[at, :] = d_up

        def give(i, carry):
            q = lax.rem(y + 2 + i, NY)
            part = pl.ds(pl.multiple_of(q * quarter, quarter), quarter)
            value = dot(d_gate, r.gate[part, :], 1, 1) + dot(d_up, r.up[part, :], 1, 1)
            r.part[q, chunk(k)] = value.astype(BF16).reshape(rows, per, quarter)
            return carry

        give(0, 0)
        remote(
            r.part.at[y_far, pl.ds(k * rows, half)],
            r.near_l.at[k], r.back_sem, r.a_l.at[k], right,
        )
        remote(
            r.part.at[y_far, pl.ds(k * rows + half, half)],
            r.near_r.at[k], r.back_sem, r.a_r.at[k], left,
        )
        lax.fori_loop(1, NY, give, 0)
        remote(
            r.part.at[y_right, pl.ds(k * rows + half, half)],
            r.last_l.at[k, pl.ds(half, half)], r.back_sem, r.b_l.at[k], right,
        )
        remote(
            r.part.at[y_left, pl.ds(k * rows, half)],
            r.last_r.at[k, pl.ds(0, half)], r.back_sem, r.b_r.at[k], left,
        )

    def second(k):
        settle(r.near_l.at[k], r.a_l.at[k])
        r.sum_r[k] = (
            r.part[y_right, pl.ds(k * rows, half)].astype(F32) + r.near_l[k].astype(F32)
        ).astype(BF16)
        remote(r.sum_r.at[k], r.last_l.at[k, pl.ds(0, half)], r.back_sem, r.b_l.at[k], right)
        settle(r.near_r.at[k], r.a_r.at[k])
        r.sum_l[k] = (
            r.part[y_left, pl.ds(k * rows + half, half)].astype(F32) + r.near_r[k].astype(F32)
        ).astype(BF16)
        remote(r.sum_l.at[k], r.last_r.at[k, pl.ds(half, half)], r.back_sem, r.b_r.at[k], left)

    def third(k, begin):
        settle(r.last_l.at[k], r.b_l.at[k])
        settle(r.last_r.at[k], r.b_r.at[k])
        r.done[k] = (
            r.part[y, chunk(k)].astype(F32)
            + r.last_l[k].astype(F32)
            + r.last_r[k].astype(F32)
        ).astype(BF16)
        zz = lax.rem(z + offset(k, nz) + nz, nz)

        def home(j, carry):
            to = lax.rem(row + j, rows)
            remote(r.done.at[k, to], r.ret.at[me], r.home_sem, r.ret_sem, target(nx, zz, to, y))
            return carry

        lax.fori_loop(begin, rows, home, 0)

    def arrive(k):
        settle(r.rows.at[y, pl.ds(0, rows)], r.come.at[k])
        spread(k)

    arrive(1)

    def step(t, carry):
        @pl.when(t + 1 <= ring)
        def _():
            arrive(t + 1)

        @pl.when(t <= ring)
        def _():
            onward(t)

        @pl.when(t == 1)
        def _():
            settle(r.rows.at[0, pl.ds(0, NY * (rows - 1))], r.come.at[0])

        @pl.when((t > 1) & (t <= ring + 1))
        def _():
            gathered(t - 1)

        @pl.when(t > ring + 1)
        def _():
            settle(r.rows.at[0, pl.ds(0, NY * rows)], r.come.at[t - 1])

        expert(t - 1)

        @pl.when(t >= 2)
        def _():
            second(t - 2)

        @pl.when(t == 2)
        def _():
            forward_row()

        @pl.when(t == nz // 2 + 1)
        def _():
            forward_z()

        @pl.when(t == 3)
        def _():
            third(0, 1)
            home = pltpu.make_async_copy(r.done.at[0, row], r.ret.at[me], r.own_sem.at[1])
            home.start()
            home.wait()

        @pl.when(t >= 4)
        def _():
            third(t - 3, 0)

        return carry

    lax.fori_loop(1, nz + 1, step, 0)

    def routed_of(q, lower):
        return r.rows[q, :, :, lower : lower + quarter].reshape(slots, quarter)

    def grads(kind, q):
        part = slice(q * quarter, (q + 1) * quarter)
        if kind == "down":
            r.g_down[:, part] = dot(r.hidden[...], routed_of(q, quarter), 0, 0).astype(BF16)
        else:
            routed = routed_of(q, 0)
            r.g_gate[part, :] = dot(routed, r.d_gate[...], 0, 0).astype(BF16)
            r.g_up[part, :] = dot(routed, r.d_up[...], 0, 0).astype(BF16)

    grads("down", 0)
    grads("down", 1)
    second(nz - 1)
    third(nz - 2, 0)
    grads("down", 2)
    grads("down", 3)
    down_out = pltpu.make_async_copy(r.g_down, r.g_down_hbm, r.own_sem.at[2])
    down_out.start()
    third(nz - 1, 0)
    for q in range(NY):
        grads("both", q)
    gate_out = pltpu.make_async_copy(r.g_gate, r.g_gate_hbm, r.own_sem.at[3])
    up_out = pltpu.make_async_copy(r.g_up, r.g_up_hbm, r.own_sem.at[4])
    gate_out.start()
    up_out.start()
    settle(r.ret.at[pl.ds(0, nz * rows - 1)], r.ret_sem)

    pieces, length = r.tg.shape[1], r.tg.shape[2]
    mid = length // 2
    returned = r.ret[...].reshape(slots, quarter)
    for i in range(pieces):
        at = slice(i * length, (i + 1) * length)
        sums = dot(r.pick[:, at], returned, 0, 0)
        r.tg[y, i] = (r.cot_q[at, :].astype(F32) + sums).astype(BF16)
        block = r.tg.at[y, i]
        remote(block, block, r.tg_sem, r.t_l.at[i], right)
        remote(block, block, r.tg_sem, r.t_r.at[i], left)

    per_sp = r.gw.shape[4]
    deep_z = r.gw.shape[3]
    many = quarter // per_sp

    def mixed(q):
        return dot(
            r.tg[q].reshape(tok, quarter),
            r.ow[pl.ds(pl.multiple_of(q * quarter, quarter), quarter), :], 1, 0,
        )

    def out_part(q):
        grad = dot(r.tg[q].reshape(tok, quarter), r.mix[...], 0, 0).astype(BF16)
        for m in range(many):
            r.gw[q, m % 2, (m // 2) % nx, m // rows] = grad[m * per_sp : (m + 1) * per_sp]
        remote(r.gw.at[q, 1 - c], r.core_in.at[q], r.core_sem, r.g1.at[q], (z, x, 1 - c, y))

    def over_x(q):
        settle(r.core_in.at[q], r.g1.at[q])
        r.x_out[q] = (r.gw[q, c].astype(F32) + r.core_in[q].astype(F32)).astype(BF16)

        def x_send(j, carry):
            to = lax.rem(x + j, nx)
            remote(r.x_out.at[q, to], r.x_in.at[q, x], r.x_sem, r.g2.at[q], (z, to, c, y))
            return carry

        lax.fori_loop(1, nx, x_send, 0)

    def over_z(q):
        if nx > 1:
            settle(r.x_in.at[q, pl.ds(0, nx - 1)], r.g2.at[q])
        total = r.x_out[q, x].astype(F32)
        for j in range(1, nx):
            total = total + r.x_in[q, lax.rem(x + j, nx)].astype(F32)
        r.last_out[pl.ds(q * deep_z, deep_z)] = total.astype(BF16)

    value = mixed(y)
    out_part(y)

    def tg_onward(i, carry):
        settle(r.tg.at[y_left, i], r.t_l.at[i])
        block = r.tg.at[y_left, i, pl.ds(0, mid)]
        remote(block, block, r.tg_sem, r.u_l.at[i], right)
        settle(r.tg.at[y_right, i], r.t_r.at[i])
        block = r.tg.at[y_right, i, pl.ds(mid, mid)]
        remote(block, block, r.tg_sem, r.u_r.at[i], left)
        return carry

    lax.fori_loop(0, pieces, tg_onward, 0)
    value = value + mixed(y_left) + mixed(y_right)
    out_part(y_left)
    out_part(y_right)
    over_x(y)

    def tg_finish(i, carry):
        settle(r.tg.at[y, i, pl.ds(0, mid)], r.u_l.at[i])
        settle(r.tg.at[y, i, pl.ds(0, mid)], r.u_r.at[i])
        return carry

    lax.fori_loop(0, pieces, tg_finish, 0)
    r.dmix[...] = (value + mixed(y_far)).astype(BF16)

    pull = jnp.zeros((256, 128), F32)
    for b in reversed(range(blocks)):
        at = slice(b * BLOCK, (b + 1) * BLOCK)
        cum = r.cum[at, :]
        end = cum[BLOCK - 1 : BLOCK, :]
        asked = (r.q[at, :].astype(F32) * 0.125 * jnp.exp(cum)).astype(BF16)
        pulled = jnp.where(same, dot(r.dmix[at, :], asked, 0, 0), 0.0)
        r.pulled[b] = pulled
        pull = pull * jnp.exp(end) + pulled
    pull = pull[0:128] + pull[128:256]
    for i in range(rows):
        r.pay[i] = pull[i * span : (i + 1) * span]

    def row_send(j, carry):
        to = lax.rem(row + j, rows)
        remote(r.pay.at[to], r.row_in.at[row], r.sent.at[0], r.p1, target(nx, z, to, y))
        return carry

    lax.fori_loop(1, rows, row_send, 0)
    out_part(y_far)
    over_x(y_left)
    over_x(y_right)
    r.row_in[row] = r.pay[row]
    inside(r, blocks)
    over_x(y_far)

    settle(r.row_in.at[pl.ds(0, rows - 1)], r.p1)
    pull = jnp.zeros((span, 128), F32)
    for j in reversed(range(rows)):
        r.row_out[j] = pull
        pull = pull * jnp.exp(kept_row(j)) + r.row_in[j]
    r.z_out[...] = pull
    r.z_in[z] = pull

    def z_send(j, carry):
        to = lax.rem(z + j, nz)
        remote(r.z_out, r.z_in.at[z], r.sent.at[1], r.p2, target(nx, to, row, y))
        return carry

    lax.fori_loop(1, nz, z_send, 0)

    for q in range(NY):
        over_z(q)

    def last_send(j, carry):
        to = lax.rem(z + j, nz)
        remote(r.last_out.at[to], r.last_in.at[z], r.sent.at[5], r.g3, (to, x, c, y))
        return carry

    lax.fori_loop(1, nz, last_send, 0)

    settle(r.z_in.at[pl.ds(0, nz - 1)], r.p2)
    pull = jnp.zeros((span, 128), F32)
    mine = jnp.zeros((span, 128), F32)
    for k in reversed(range(nz)):
        mine = jnp.where(z == k, pull, mine)
        pull = pull * jnp.exp(kept_z(k)) + r.z_in[k]
    behind = jnp.zeros((1, 128), F32)
    for j in reversed(range(rows)):
        r.row_out[j] = r.row_out[j] + mine * jnp.exp(behind)
        behind = behind + kept_row(j)

    def row_back(j, carry):
        to = lax.rem(row + j, rows)
        remote(r.row_out.at[to], r.ex.at[row], r.sent.at[2], r.p3, target(nx, z, to, y))
        return carry

    lax.fori_loop(1, rows, row_back, 0)
    r.ex[row] = r.row_out[row]

    settle(r.f_ex.at[pl.ds(0, rows - 1)], r.f3)
    settle(r.ex.at[pl.ds(0, rows - 1)], r.p3)
    across(r, blocks, rows, same)

    settle(r.last_in.at[pl.ds(0, nz - 1)], r.g3)
    total = r.last_out[z].astype(F32)
    for j in range(1, nz):
        total = total + r.last_in[lax.rem(z + j, nz)].astype(F32)
    r.gout[...] = total

    settle(r.send.at[pl.ds(0, ring * rows)], r.send_sem)
    settle(r.full.at[pl.ds(0, (1 + TRAIL) * rows - 1)], r.full_sem)
    settle(r.rows.at[pl.ds(0, 3), pl.ds(0, ring * rows)], r.ring_sem)
    settle(r.part.at[pl.ds(0, 3)], r.back_sem)
    settle(r.ret.at[pl.ds(0, nz * rows - 1)], r.home_sem)
    settle(r.tg.at[pl.ds(0, 3)], r.tg_sem)
    settle(r.pay.at[pl.ds(0, rows - 1)], r.sent.at[0])
    settle(r.z_in.at[pl.ds(0, nz - 1)], r.sent.at[1])
    settle(r.ex.at[pl.ds(0, rows - 1)], r.sent.at[2])
    settle(r.f_pay.at[pl.ds(0, rows - 1)], r.f_sent.at[0])
    settle(r.f_z_in.at[pl.ds(0, nz - 1)], r.f_sent.at[1])
    settle(r.f_ex.at[pl.ds(0, rows - 1)], r.f_sent.at[2])
    settle(r.core_in, r.core_sem)
    settle(r.last_in.at[pl.ds(0, nz - 1)], r.sent.at[5])
    if nx > 1:
        settle(r.x_in.at[:, pl.ds(0, nx - 1)], r.x_sem)
    down_out.wait()
    gate_out.wait()
    up_out.wait()


def inside(r, blocks):
    head0 = lax.broadcasted_iota(jnp.int32, (BLOCK, 128), 1) < 64
    le = triangle("le")
    ge = triangle("ge").astype(BF16)
    for b in range(blocks):
        at = slice(b * BLOCK, (b + 1) * BLOCK)
        cum = r.cum[at, :]
        middle = cum[BLOCK // 2 - 1 : BLOCK // 2, :]
        up, down = jnp.exp(cum - middle), jnp.exp(middle - cum)
        q_mid = (r.q[at, :].astype(F32) * 0.125 * up).astype(BF16)
        k_mid = (r.k[at, :].astype(F32) * down).astype(BF16)
        nothing = jnp.zeros_like(q_mid)
        dq_mid = jnp.zeros((BLOCK, 128), F32)
        dk_mid = jnp.zeros((BLOCK, 128), F32)
        for h in range(2):
            cols = slice(h * 128, (h + 1) * 128)
            mine = head0 if h == 0 else jnp.logical_not(head0)
            q_one = jnp.where(mine, q_mid, nothing)
            k_one = jnp.where(mine, k_mid, nothing)
            cot = r.dmix[at, cols]
            scores = jnp.where(le, dot(q_one, k_one, 1, 1), 0.0).astype(BF16)
            d_scores = jnp.where(le, dot(cot, r.v[at, cols], 1, 1), 0.0).astype(BF16)
            dq_mid = dq_mid + dot(d_scores, k_one, 1, 0)
            dk_mid = dk_mid + dot(d_scores, q_one, 0, 0)
            r.dv_in[at, cols] = dot(scores, cot, 0, 0)
        r.dq_in[at, :] = dq_mid * up
        r.dk_in[at, :] = dk_mid * down
        r.dl_in[at, :] = spread_sum(ge, q_mid.astype(F32) * dq_mid - k_mid.astype(F32) * dk_mid)


def across(r, blocks, rows, same):
    ge = triangle("ge").astype(BF16)
    lt = triangle("lt").astype(BF16)

    def opened(ref):
        compact = jnp.concatenate([ref[i] for i in range(rows)], axis=0)
        return jnp.where(same, jnp.concatenate([compact, compact], axis=0), 0.0)

    def end_of(b):
        return jnp.exp(r.cum[(b + 1) * BLOCK - 1 : (b + 1) * BLOCK, :])

    states = [opened(r.f_ex)]
    for b in range(blocks - 1):
        states.append(states[-1] * end_of(b) + r.added[b])
    pulls = [opened(r.ex)]
    for b in reversed(range(1, blocks)):
        pulls.insert(0, pulls[0] * end_of(b) + r.pulled[b])
    for b in range(blocks):
        at = slice(b * BLOCK, (b + 1) * BLOCK)
        cum = r.cum[at, :]
        end = cum[BLOCK - 1 : BLOCK, :]
        query = r.q[at, :].astype(F32) * 0.125
        key = r.k[at, :].astype(F32)
        asked, kept = jnp.exp(cum), jnp.exp(end - cum)
        pull = pulls[b].astype(BF16)
        far_v = dot((key * kept).astype(BF16), pull, 1, 1)
        r.dv[at, :] = (r.dv_in[at, :] + far_v).astype(BF16)
        dq_far = dot(r.dmix[at, :], states[b].astype(BF16), 1, 0) * asked
        dk_far = dot(r.v[at, :], pull, 1, 0) * kept
        r.dq[at, :] = ((r.dq_in[at, :] + dq_far) * 0.125).astype(BF16)
        r.dk[at, :] = (r.dk_in[at, :] + dk_far).astype(BF16)
        carried = jnp.sum(states[b] * pulls[b], axis=0, keepdims=True) * jnp.exp(end)
        r.dl[at, :] = (
            r.dl_in[at, :] + spread_sum(ge, query * dq_far) + spread_sum(lt, key * dk_far) + carried
        )


class Refs:
    pass


def mega(ids, weights, moe, cot, gate, up, down, out_weight, mix, query, key, value, log_decay):
    nz, nx = sizes()
    rows = 2 * nx
    half = rows // 2
    tok, width = moe.shape
    quarter = width // NY
    experts = nz * rows
    per = 2 * tok // experts
    span = 128 // rows
    deep = span + 8
    per_sp = width // experts
    units = gate.shape[1]
    sem = pltpu.SemaphoreType.DMA

    def vm(*shape, dtype=BF16):
        return pltpu.VMEM(shape, dtype)

    ins = [
        "ids",
        "weights",
        "moe_hbm",
        "cot_hbm",
        "gate_hbm",
        "up_hbm",
        "down_hbm",
        "ow_hbm",
        "mix_hbm",
        "q_hbm",
        "k_hbm",
        "v_hbm",
        "ld_hbm",
    ]
    outs = {
        "g_gate_hbm": (gate.shape, BF16),
        "g_up_hbm": (up.shape, BF16),
        "g_down_hbm": (down.shape, BF16),
        "gout": ((per_sp, 256), F32),
        "dq": ((tok, 128), BF16),
        "dk": ((tok, 128), BF16),
        "dv": ((tok, 256), BF16),
        "dl": ((tok, 128), F32),
    }
    scratch = {
        "moe_q": vm(tok, quarter),
        "cot_q": vm(tok, quarter),
        "ld": vm(tok, 128, dtype=F32),
        "k": vm(tok, 128),
        "v": vm(tok, 256),
        "q": vm(tok, 128),
        "gate": vm(*gate.shape),
        "up": vm(*up.shape),
        "down": vm(*down.shape),
        "ow": vm(*out_weight.shape),
        "mix": vm(*mix.shape),
        "pick": vm(2 * tok, tok),
        "send": vm(experts, per, 2 * quarter),
        "rows": vm(NY, experts, per, 2 * quarter),
        "hidden": vm(2 * tok, units),
        "d_gate": vm(2 * tok, units),
        "d_up": vm(2 * tok, units),
        "part": vm(NY, experts, per, quarter),
        "near_l": vm(nz, half, per, quarter),
        "near_r": vm(nz, half, per, quarter),
        "sum_l": vm(nz, half, per, quarter),
        "sum_r": vm(nz, half, per, quarter),
        "last_l": vm(nz, rows, per, quarter),
        "last_r": vm(nz, rows, per, quarter),
        "done": vm(nz, rows, per, quarter),
        "ret": vm(experts, per, quarter),
        "g_gate": vm(*gate.shape),
        "g_up": vm(*up.shape),
        "g_down": vm(*down.shape),
        "tg": vm(NY, 4, tok // 4, quarter),
        "dmix": vm(tok, 256),
        "cum": vm(tok, 128, dtype=F32),
        "added": vm(tok // BLOCK, 256, 128, dtype=F32),
        "pulled": vm(tok // BLOCK, 256, 128, dtype=F32),
        "dv_in": vm(tok, 256, dtype=F32),
        "dq_in": vm(tok, 128, dtype=F32),
        "dk_in": vm(tok, 128, dtype=F32),
        "dl_in": vm(tok, 128, dtype=F32),
        "moe": vm(tok, width),
        "cot": vm(tok, width),
        "slot_weight": vm(2 * tok, 128, dtype=F32),
        "full": vm((1 + TRAIL) * rows, NY, per, 2 * quarter),
        "gw": vm(NY, 2, nx, nz // NY, per_sp, 256),
        "f_pay": vm(rows, deep, 128, dtype=F32),
        "f_row_in": vm(rows, deep, 128, dtype=F32),
        "f_z_out": vm(deep, 128, dtype=F32),
        "f_z_in": vm(nz, deep, 128, dtype=F32),
        "f_row_out": vm(rows, span, 128, dtype=F32),
        "f_ex": vm(rows, span, 128, dtype=F32),
        "pay": vm(rows, span, 128, dtype=F32),
        "row_in": vm(rows, span, 128, dtype=F32),
        "z_out": vm(span, 128, dtype=F32),
        "z_in": vm(nz, span, 128, dtype=F32),
        "row_out": vm(rows, span, 128, dtype=F32),
        "ex": vm(rows, span, 128, dtype=F32),
        "core_in": vm(NY, nx, nz // NY, per_sp, 256),
        "x_out": vm(NY, nx, nz // NY, per_sp, 256),
        "x_in": vm(NY, nx, nz // NY, per_sp, 256),
        "last_out": vm(nz, per_sp, 256),
        "last_in": vm(nz, per_sp, 256),
        "ends": vm(rows, 128, dtype=F32),
        "load_sem": sem((13,)),
        "own_sem": sem((5,)),
        "sent": sem((6,)),
        "f_sent": sem((3,)),
    }
    for name in ("send_sem", "ring_sem", "back_sem", "home_sem", "ret_sem", "tg_sem", "p1", "p2", "p3", "g3", "full_sem", "core_sem", "x_sem", "f1", "f2", "f3"):
        scratch[name] = sem
    for name in ("come", "from_l", "from_r", "far_l", "far_r", "a_l", "a_r", "b_l", "b_r"):
        scratch[name] = sem((nz,))
    for name in ("t_l", "t_r", "u_l", "u_r", "g1", "g2"):
        scratch[name] = sem((4,))
    names = ins + list(outs) + list(scratch)

    def body(*refs):
        r = Refs()
        for name, ref in zip(names, refs):
            setattr(r, name, ref)
        mega_kernel(r, nz, nx)

    return pl.pallas_call(
        body,
        name="mega",
        out_shape=tuple(jax.ShapeDtypeStruct(*kind) for kind in outs.values()),
        in_specs=[VMEM, VMEM] + [ANY] * 11,
        out_specs=(ANY,) * 3 + (VMEM,) * 5,
        scratch_shapes=list(scratch.values()),
        compiler_params=params(1),
    )(ids, weights, moe, cot, gate, up, down, out_weight, mix, query, key, value, log_decay)


def finish_kernel(*refs):
    count = (len(refs) - 1) // 3
    sources, results, held, sem = (
        refs[:count],
        refs[count : 2 * count],
        refs[2 * count : 3 * count],
        refs[-1],
    )
    inward = [pltpu.make_async_copy(a, b, sem.at[0, i]) for i, (a, b) in enumerate(zip(sources, held))]
    outward = [pltpu.make_async_copy(a, b, sem.at[1, i]) for i, (a, b) in enumerate(zip(held, results))]
    for copy in inward:
        copy.start()
    for one, other in zip(inward, outward):
        one.wait()
        other.start()
    for copy in outward:
        copy.wait()


def finish(arrays):
    shapes = tuple(jax.ShapeDtypeStruct(a.shape, a.dtype) for a in arrays)
    return pl.pallas_call(
        finish_kernel,
        name="finish",
        out_shape=shapes,
        in_specs=[ANY] * len(arrays),
        out_specs=(ANY,) * len(arrays),
        scratch_shapes=[pltpu.VMEM(a.shape, a.dtype) for a in arrays]
        + [pltpu.SemaphoreType.DMA((2, len(arrays)))],
        compiler_params=params(),
    )(*arrays)


def shards(
    moe_input,
    cotangent,
    expert_ids,
    route_weights,
    gate_weight,
    up_weight,
    down_weight,
    out_weight,
    mixer_out,
    query_vectors,
    key_vectors,
    value_vectors,
    log_decay,
):
    results = mega(
        expert_ids.T,
        route_weights.T,
        moe_input,
        cotangent,
        gate_weight[0],
        up_weight[0],
        down_weight[0],
        out_weight,
        mixer_out,
        query_vectors,
        key_vectors,
        value_vectors,
        log_decay,
    )
    g_gate, g_up, g_down, gout, dq, dk, dv, dl = finish(results)
    return g_gate[None], g_up[None], g_down[None], gout, dq, dk, dv, dl


def solution(mesh):
    finer = Mesh(mesh.devices.reshape(8, 4, 2, mesh.shape["tp"]), ("sp_0", "sp_1", "sp_2", "tp"))
    in_specs = (
        P(SP, None),
        P(SP, None),
        P(SP, None),
        P(SP, None),
        P(SP, None, "tp"),
        P(SP, None, "tp"),
        P(SP, "tp", None),
        P(None, "tp"),
        P(SP, "tp"),
        P(SP, "tp"),
        P(SP, "tp"),
        P(SP, "tp"),
        P(SP, "tp"),
    )
    out_specs = (
        P(SP, None, "tp"),
        P(SP, None, "tp"),
        P(SP, "tp", None),
        P(SP, "tp"),
        P(SP, "tp"),
        P(SP, "tp"),
        P(SP, "tp"),
        P(SP, "tp"),
    )
    return jax.shard_map(
        shards, mesh=finer, in_specs=in_specs, out_specs=out_specs, check_vma=False
    )
```

```python
import jax
import jax.numpy as jnp
from jax import lax
from jax.experimental import pallas as pl
from jax.experimental.pallas import tpu as pltpu
from jax.sharding import Mesh
from jax.sharding import PartitionSpec as P

MESH = pl.DeviceIdType.MESH
SP = ("sp_0", "sp_1", "sp_2")
BF16 = jnp.bfloat16
F32 = jnp.float32
NY = 4
FULL = {8: (5, 7)}
ORDER = {8: (0, 2, 6, 3, 5, 1, 4, 7)}
BLOCK = 64
VMEM = pl.BlockSpec(memory_space=pltpu.VMEM)
ANY = pl.BlockSpec(memory_space=pl.ANY)


def sizes():
    return lax.axis_size("sp_0"), lax.axis_size("sp_1")


def params(collective_id=None):
    if collective_id is None:
        return pltpu.CompilerParams(vmem_limit_bytes=60 * 1024 * 1024)
    return pltpu.CompilerParams(
        collective_id=collective_id, has_side_effects=True, vmem_limit_bytes=60 * 1024 * 1024
    )


def dot(a, b, ca, cb):
    return lax.dot_general(a, b, (((ca,), (cb,)), ((), ())), preferred_element_type=F32)


def place():
    return (
        lax.axis_index("sp_0"),
        lax.axis_index("sp_1"),
        lax.axis_index("sp_2"),
        lax.axis_index("tp"),
    )


def target(nx, zz, row, y):
    return (zz, row // 2, row % 2, y)


def offset(k, nz):
    order = ORDER.get(nz, tuple(range(nz)))
    out = 0
    for i, ahead in enumerate(order):
        out = out + jnp.where(k == i, ahead, 0)
    return out


def settle(ref, sem):
    pltpu.make_async_copy(ref, ref, sem).wait()


def greet_plane(barrier, nz, nx, z, x, c, y):
    def hello(device):
        pl.semaphore_signal(barrier, inc=1, device_id=device, device_id_type=MESH)

    columns = [lax.rem(x + i, nx) for i in range(nx)]

    def level(zz, own):
        for i in reversed(range(nx)):
            hello((zz, columns[i], 1 - c, y))
            if i or not own:
                hello((zz, columns[i], c, y))

    def level_at(i, carry):
        away = jnp.where(i % 2 == 0, nz // 2 - i // 2, nz // 2 + 1 + i // 2)
        level(lax.rem(z + away, nz), False)
        return carry

    lax.fori_loop(0, nz - 1, level_at, 0)
    level(z, True)
    for side in (1, NY - 1):
        hello((z, x, c, lax.rem(y + side, NY)))


def remote(src, dst, send_sem, recv_sem, device):
    copy = pltpu.make_async_remote_copy(
        src_ref=src,
        dst_ref=dst,
        send_sem=send_sem,
        recv_sem=recv_sem,
        device_id=device,
        device_id_type=MESH,
    )
    copy.start()


def triangle(kind):
    row = lax.broadcasted_iota(jnp.int32, (BLOCK, BLOCK), 0)
    col = lax.broadcasted_iota(jnp.int32, (BLOCK, BLOCK), 1)
    return {"le": col <= row, "ge": col >= row, "lt": col < row}[kind]


def spread_sum(tri, value):
    high = value.astype(BF16)
    rest = value - high.astype(F32)
    mid = rest.astype(BF16)
    low = (rest - mid.astype(F32)).astype(BF16)
    both = jnp.concatenate([high, mid, low], axis=0)
    return dot(jnp.concatenate([tri, tri, tri], axis=1), both, 1, 0)


def diagonal(shape):
    return (lax.broadcasted_iota(jnp.int32, shape, 0) < shape[0] // 2) == (
        lax.broadcasted_iota(jnp.int32, shape, 1) < shape[1] // 2
    )


def mega_kernel(r, nz, nx):
    z, x, c, y = place()
    rows = 2 * nx
    row = x * 2 + c
    me = z * rows + row
    half = rows // 2
    tok, quarter = r.moe_q.shape
    experts, per = nz * rows, 2 * tok // (nz * rows)
    slots = 2 * tok
    units = r.gate.shape[1]
    y_left, y_right = lax.rem(y + NY - 1, NY), lax.rem(y + 1, NY)
    y_far = lax.rem(y + 2, NY)
    right = target(nx, z, row, y_right)
    left = target(nx, z, row, y_left)
    cols = pl.ds(pl.multiple_of(y * quarter, quarter), quarter)
    loads = [
        pltpu.make_async_copy(src, dst, r.load_sem.at[i])
        for i, (src, dst) in enumerate(
            (
                (r.ids_hbm, r.ids),
                (r.weights_hbm, r.weights),
                (r.moe_hbm.at[:, cols], r.moe_q),
                (r.cot_hbm.at[:, cols], r.cot_q),
                (r.ld_hbm, r.ld),
                (r.k_hbm, r.k),
                (r.v_hbm, r.v),
                (r.gate_hbm, r.gate),
                (r.up_hbm, r.up),
                (r.down_hbm, r.down),
                (r.q_hbm, r.q),
                (r.ow_hbm, r.ow),
                (r.mix_hbm, r.mix),
                (r.moe_hbm, r.moe),
                (r.cot_hbm, r.cot),
            )
        )
    ]
    for load in loads[:4]:
        load.start()
    barrier = pltpu.get_barrier_semaphore()
    greet_plane(barrier, nz, nx, z, x, c, y)

    for load in loads[4:]:
        load.start()
    for load in loads[:2]:
        load.wait()
    lanes = max(128, experts)
    which = lax.broadcasted_iota(jnp.int32, (lanes, tok), 0)
    hot = [(r.ids[j : j + 1, :] == which).astype(F32) for j in range(2)]
    earlier = (
        lax.broadcasted_iota(jnp.int32, (tok, tok), 0)
        < lax.broadcasted_iota(jnp.int32, (tok, tok), 1)
    ).astype(BF16)
    before = dot((hot[0] + hot[1]).astype(BF16), earlier, 1, 0)
    slot_iota = lax.broadcasted_iota(jnp.int32, (slots, tok), 0)
    picks = []
    for j in range(2):
        rank = jnp.sum(before * hot[j], axis=0, keepdims=True).astype(jnp.int32)
        slot = r.ids[j : j + 1, :] * per + rank
        picks.append((slot == slot_iota).astype(BF16))
    both = picks[0] + picks[1]
    r.pick[...] = both
    slot_weight = jnp.zeros((slots, 1), F32)
    for j in range(2):
        chosen = picks[j].astype(F32) * r.weights[j : j + 1, :]
        slot_weight = slot_weight + jnp.sum(chosen, axis=1, keepdims=True)
    r.slot_weight[...] = jnp.broadcast_to(slot_weight, (slots, 128))
    loads[2].wait()
    sorted_rows = dot(both, r.moe_q[...], 1, 0).astype(BF16)
    r.send[:, :, 0:quarter] = sorted_rows.reshape(experts, per, quarter)
    loads[3].wait()
    sorted_cot = (dot(both, r.cot_q[...], 1, 0) * slot_weight).astype(BF16)
    r.send[:, :, quarter:] = sorted_cot.reshape(experts, per, quarter)
    pl.semaphore_wait(barrier, nz * rows + 1)

    def scatter(i, carry):
        k, j = i // rows, lax.rem(i, rows)
        zz = lax.rem(z - offset(k, nz) + nz, nz)
        to = lax.rem(row + j, rows)
        remote(
            r.send.at[zz * rows + to],
            r.rows.at[y, k * rows + row],
            r.send_sem,
            r.come.at[k],
            target(nx, zz, to, y),
        )
        return carry

    own = pltpu.make_async_copy(r.send.at[me], r.rows.at[y, row], r.own_sem.at[0])
    own.start()
    wide = FULL.get(nz, (nz - 1,))
    ringed = [k for k in range(nz) if k not in wide]
    lines = rows * per

    def fill(i, k):
        zz = lax.rem(z - offset(k, nz) + nz, nz)
        there = pl.ds(pl.multiple_of(zz * lines, lines), lines)
        pick_there = r.pick[there, :]
        weight_there = r.slot_weight[there, 0:1]
        block = slice(i * rows, (i + 1) * rows)
        for q in range(NY):
            part = slice(q * quarter, (q + 1) * quarter)
            value = dot(pick_there, r.moe[:, part], 1, 0).astype(BF16)
            r.full[block, q, :, 0:quarter] = value.reshape(rows, per, quarter)
            value = (dot(pick_there, r.cot[:, part], 1, 0) * weight_there).astype(BF16)
            r.full[block, q, :, quarter:] = value.reshape(rows, per, quarter)

    def scatter_full(i, k):
        zz = lax.rem(z - offset(k, nz) + nz, nz)

        def one(j, carry):
            to = lax.rem(row + j, rows)
            remote(
                r.full.at[i * rows + to],
                r.rows.at[:, k * rows + row],
                r.full_sem,
                r.come.at[k],
                target(nx, zz, to, y),
            )
            return carry

        lax.fori_loop(0, rows, one, 0)

    begin = 1
    for i, k in enumerate(wide):
        lax.fori_loop(begin, k * rows, scatter, 0)
        if i == 0:
            loads[13].wait()
            loads[14].wait()
            for ii, kk in enumerate(wide):
                fill(ii, kk)
        scatter_full(i, k)
        begin = (k + 1) * rows
    if begin < nz * rows:
        lax.fori_loop(begin, nz * rows, scatter, 0)
    own.wait()

    def is_ring(k):
        answer = k >= 0
        for w in wide:
            answer = answer & (k != w)
        return answer

    blocks = tok // BLOCK
    same = diagonal((256, 128))
    tri = triangle("le").astype(BF16)
    for load in loads[4:7]:
        load.wait()
    state = jnp.zeros((256, 128), F32)
    for b in range(blocks):
        at = slice(b * BLOCK, (b + 1) * BLOCK)
        cum = spread_sum(tri, r.ld[at, :])
        r.cum[at, :] = cum
        end = cum[BLOCK - 1 : BLOCK, :]
        kept = (r.k[at, :].astype(F32) * jnp.exp(end - cum)).astype(BF16)
        added = jnp.where(same, dot(r.v[at, :], kept, 0, 0), 0.0)
        r.added[b] = added
        state = state * jnp.exp(end) + added
        whole = end if b == 0 else whole + end
    state = state[0:128] + state[128:256]
    span = 128 // rows
    for i in range(rows):
        r.f_pay[i, 0:span, :] = state[i * span : (i + 1) * span]
        r.f_pay[i, span:, :] = jnp.broadcast_to(whole, (8, 128))

    def f_send(j, carry):
        to = lax.rem(row + j, rows)
        remote(r.f_pay.at[to], r.f_row_in.at[row], r.f_sent.at[0], r.f1, target(nx, z, to, y))
        return carry

    lax.fori_loop(1, rows, f_send, 0)
    r.f_row_in[row] = r.f_pay[row]

    def kept_row(j):
        return r.f_row_in[j, span : span + 1, :]

    def kept_z(k):
        return r.f_z_in[k, span : span + 1, :]

    def forward_row():
        settle(r.f_row_in.at[pl.ds(0, rows - 1)], r.f1)
        state = jnp.zeros((span, 128), F32)
        after = jnp.zeros((1, 128), F32)
        for j in range(rows):
            r.f_row_out[j] = state
            r.ends[j : j + 1, :] = after
            state = state * jnp.exp(kept_row(j)) + r.f_row_in[j, 0:span, :]
            after = after + kept_row(j)
        r.f_z_out[0:span, :] = state
        r.f_z_out[span:, :] = jnp.broadcast_to(after, (8, 128))
        r.f_z_in[z] = r.f_z_out[...]

        def send(j, carry):
            to = lax.rem(z + j, nz)
            remote(r.f_z_out, r.f_z_in.at[z], r.f_sent.at[1], r.f2, target(nx, to, row, y))
            return carry

        lax.fori_loop(1, nz, send, 0)

    def forward_z():
        settle(r.f_z_in.at[pl.ds(0, nz - 1)], r.f2)
        state = jnp.zeros((span, 128), F32)
        mine = jnp.zeros((span, 128), F32)
        for k in range(nz):
            mine = jnp.where(z == k, state, mine)
            state = state * jnp.exp(kept_z(k)) + r.f_z_in[k, 0:span, :]
        for j in range(rows):
            r.f_row_out[j] = r.f_row_out[j] + mine * jnp.exp(r.ends[j : j + 1, :])

        def send(j, carry):
            to = lax.rem(row + j, rows)
            remote(r.f_row_out.at[to], r.f_ex.at[row], r.f_sent.at[2], r.f3, target(nx, z, to, y))
            return carry

        lax.fori_loop(1, rows, send, 0)
        r.f_ex[row] = r.f_row_out[row]

    for load in loads[7:13]:
        load.wait()

    def chunk(k):
        return pl.ds(k * rows, rows)

    def spread(k):
        block = r.rows.at[y, chunk(k)]
        remote(block, block, r.ring_sem, r.from_l.at[k], right)
        remote(block, block, r.ring_sem, r.from_r.at[k], left)

    def onward(k):
        settle(r.rows.at[y_left, chunk(k)], r.from_l.at[k])
        block = r.rows.at[y_left, pl.ds(k * rows, half)]
        remote(block, block, r.ring_sem, r.far_l.at[k], right)
        settle(r.rows.at[y_right, chunk(k)], r.from_r.at[k])
        block = r.rows.at[y_right, pl.ds(k * rows + half, half)]
        remote(block, block, r.ring_sem, r.far_r.at[k], left)

    def gathered(k):
        settle(r.rows.at[y, pl.ds(0, half)], r.far_l.at[k])
        settle(r.rows.at[y, pl.ds(0, half)], r.far_r.at[k])

    def expert(k):
        pre_gate = jnp.zeros((lines, units), F32)
        pre_up = jnp.zeros((lines, units), F32)
        delta = jnp.zeros((lines, units), F32)
        for q in range(NY):
            part = slice(q * quarter, (q + 1) * quarter)
            routed = r.rows[q, chunk(k), :, 0:quarter].reshape(lines, quarter)
            routed_cot = r.rows[q, chunk(k), :, quarter:].reshape(lines, quarter)
            pre_gate = pre_gate + dot(routed, r.gate[part, :], 1, 0)
            pre_up = pre_up + dot(routed, r.up[part, :], 1, 0)
            delta = delta + dot(routed_cot, r.down[:, part], 1, 1)
        sig = jax.nn.sigmoid(pre_gate)
        act = pre_gate * sig
        d_gate = (delta * pre_up * sig * (1.0 + pre_gate * (1.0 - sig))).astype(BF16)
        d_up = (delta * act).astype(BF16)
        at = pl.ds(pl.multiple_of(k * lines, lines), lines)
        r.hidden[at, :] = (act * pre_up).astype(BF16)
        r.d_gate[at, :] = d_gate
        r.d_up[at, :] = d_up

        def give(i, carry):
            q = lax.rem(y + 2 + i, NY)
            part = pl.ds(pl.multiple_of(q * quarter, quarter), quarter)
            value = dot(d_gate, r.gate[part, :], 1, 1) + dot(d_up, r.up[part, :], 1, 1)
            r.part[q, chunk(k)] = value.astype(BF16).reshape(rows, per, quarter)
            return carry

        give(0, 0)
        remote(
            r.part.at[y_far, pl.ds(k * rows, half)],
            r.near_l.at[k], r.back_sem, r.a_l.at[k], right,
        )
        remote(
            r.part.at[y_far, pl.ds(k * rows + half, half)],
            r.near_r.at[k], r.back_sem, r.a_r.at[k], left,
        )
        lax.fori_loop(1, NY, give, 0)
        remote(
            r.part.at[y_right, pl.ds(k * rows + half, half)],
            r.last_l.at[k, pl.ds(half, half)], r.back_sem, r.b_l.at[k], right,
        )
        remote(
            r.part.at[y_left, pl.ds(k * rows, half)],
            r.last_r.at[k, pl.ds(0, half)], r.back_sem, r.b_r.at[k], left,
        )

    def second(k):
        settle(r.near_l.at[k], r.a_l.at[k])
        r.sum_r[k] = (
            r.part[y_right, pl.ds(k * rows, half)].astype(F32) + r.near_l[k].astype(F32)
        ).astype(BF16)
        remote(r.sum_r.at[k], r.last_l.at[k, pl.ds(0, half)], r.back_sem, r.b_l.at[k], right)
        settle(r.near_r.at[k], r.a_r.at[k])
        r.sum_l[k] = (
            r.part[y_left, pl.ds(k * rows + half, half)].astype(F32) + r.near_r[k].astype(F32)
        ).astype(BF16)
        remote(r.sum_l.at[k], r.last_r.at[k, pl.ds(half, half)], r.back_sem, r.b_r.at[k], left)

    def third(k, begin):
        settle(r.last_l.at[k], r.b_l.at[k])
        settle(r.last_r.at[k], r.b_r.at[k])
        r.done[k] = (
            r.part[y, chunk(k)].astype(F32)
            + r.last_l[k].astype(F32)
            + r.last_r[k].astype(F32)
        ).astype(BF16)
        zz = lax.rem(z + offset(k, nz) + nz, nz)

        def home(j, carry):
            to = lax.rem(row + j, rows)
            remote(r.done.at[k, to], r.ret.at[me], r.home_sem, r.ret_sem, target(nx, zz, to, y))
            return carry

        lax.fori_loop(begin, rows, home, 0)

    def arrive(k):
        settle(r.rows.at[y, pl.ds(0, rows)], r.come.at[k])
        spread(k)

    settle(r.rows.at[y, pl.ds(0, rows - 1)], r.come.at[0])
    spread(0)
    arrive(1)
    onward(0)

    def step(t, carry):
        @pl.when(is_ring(t + 1) & (t + 1 < nz))
        def _():
            arrive(t + 1)

        @pl.when(is_ring(t) & (t < nz))
        def _():
            onward(t)

        @pl.when(is_ring(t - 1))
        def _():
            gathered(t - 1)

        @pl.when(jnp.logical_not(is_ring(t - 1)))
        def _():
            settle(r.rows.at[0, pl.ds(0, NY * rows)], r.come.at[t - 1])

        expert(t - 1)

        @pl.when(t >= 2)
        def _():
            second(t - 2)

        @pl.when(t == 2)
        def _():
            forward_row()

        @pl.when(t == nz // 2 + 1)
        def _():
            forward_z()

        @pl.when(t == 3)
        def _():
            third(0, 1)
            home = pltpu.make_async_copy(r.done.at[0, row], r.ret.at[me], r.own_sem.at[1])
            home.start()
            home.wait()

        @pl.when(t >= 4)
        def _():
            third(t - 3, 0)

        return carry

    lax.fori_loop(1, nz + 1, step, 0)

    def routed_of(q, lower):
        return r.rows[q, :, :, lower : lower + quarter].reshape(slots, quarter)

    def grads(kind, q):
        part = slice(q * quarter, (q + 1) * quarter)
        if kind == "down":
            r.g_down[:, part] = dot(r.hidden[...], routed_of(q, quarter), 0, 0).astype(BF16)
        else:
            routed = routed_of(q, 0)
            r.g_gate[part, :] = dot(routed, r.d_gate[...], 0, 0).astype(BF16)
            r.g_up[part, :] = dot(routed, r.d_up[...], 0, 0).astype(BF16)

    grads("down", 0)
    grads("down", 1)
    second(nz - 1)
    third(nz - 2, 0)
    grads("down", 2)
    grads("down", 3)
    third(nz - 1, 0)
    for q in range(NY):
        grads("both", q)
    settle(r.ret.at[pl.ds(0, nz * rows - 1)], r.ret_sem)

    pieces, length = r.tg.shape[1], r.tg.shape[2]
    mid = length // 2
    returned = r.ret[...].reshape(slots, quarter)
    for i in range(pieces):
        at = slice(i * length, (i + 1) * length)
        sums = dot(r.pick[:, at], returned, 0, 0)
        r.tg[y, i] = (r.cot_q[at, :].astype(F32) + sums).astype(BF16)
        block = r.tg.at[y, i]
        remote(block, block, r.tg_sem, r.t_l.at[i], right)
        remote(block, block, r.tg_sem, r.t_r.at[i], left)

    per_sp = r.gw.shape[4]
    deep_z = r.gw.shape[3]
    many = quarter // per_sp

    def mixed(q):
        return dot(
            r.tg[q].reshape(tok, quarter),
            r.ow[pl.ds(pl.multiple_of(q * quarter, quarter), quarter), :], 1, 0,
        )

    def out_part(q):
        grad = dot(r.tg[q].reshape(tok, quarter), r.mix[...], 0, 0).astype(BF16)
        for m in range(many):
            r.gw[q, m % 2, (m // 2) % nx, m // rows] = grad[m * per_sp : (m + 1) * per_sp]
        remote(r.gw.at[q, 1 - c], r.core_in.at[q], r.core_sem, r.g1.at[q], (z, x, 1 - c, y))

    def over_x(q):
        settle(r.core_in.at[q], r.g1.at[q])
        r.x_out[q] = (r.gw[q, c].astype(F32) + r.core_in[q].astype(F32)).astype(BF16)

        def x_send(j, carry):
            to = lax.rem(x + j, nx)
            remote(r.x_out.at[q, to], r.x_in.at[q, x], r.x_sem, r.g2.at[q], (z, to, c, y))
            return carry

        lax.fori_loop(1, nx, x_send, 0)

    def over_z(q):
        if nx > 1:
            settle(r.x_in.at[q, pl.ds(0, nx - 1)], r.g2.at[q])
        total = r.x_out[q, x].astype(F32)
        for j in range(1, nx):
            total = total + r.x_in[q, lax.rem(x + j, nx)].astype(F32)
        r.last_out[pl.ds(q * deep_z, deep_z)] = total.astype(BF16)

    value = mixed(y)
    out_part(y)

    def tg_onward(i, carry):
        settle(r.tg.at[y_left, i], r.t_l.at[i])
        block = r.tg.at[y_left, i, pl.ds(0, mid)]
        remote(block, block, r.tg_sem, r.u_l.at[i], right)
        settle(r.tg.at[y_right, i], r.t_r.at[i])
        block = r.tg.at[y_right, i, pl.ds(mid, mid)]
        remote(block, block, r.tg_sem, r.u_r.at[i], left)
        return carry

    lax.fori_loop(0, pieces, tg_onward, 0)
    value = value + mixed(y_left) + mixed(y_right)
    out_part(y_left)
    out_part(y_right)
    over_x(y)

    def tg_finish(i, carry):
        settle(r.tg.at[y, i, pl.ds(0, mid)], r.u_l.at[i])
        settle(r.tg.at[y, i, pl.ds(0, mid)], r.u_r.at[i])
        return carry

    lax.fori_loop(0, pieces, tg_finish, 0)
    r.dmix[...] = (value + mixed(y_far)).astype(BF16)

    pull = jnp.zeros((256, 128), F32)
    for b in reversed(range(blocks)):
        at = slice(b * BLOCK, (b + 1) * BLOCK)
        cum = r.cum[at, :]
        end = cum[BLOCK - 1 : BLOCK, :]
        asked = (r.q[at, :].astype(F32) * 0.125 * jnp.exp(cum)).astype(BF16)
        pulled = jnp.where(same, dot(r.dmix[at, :], asked, 0, 0), 0.0)
        r.pulled[b] = pulled
        pull = pull * jnp.exp(end) + pulled
    pull = pull[0:128] + pull[128:256]
    for i in range(rows):
        r.pay[i] = pull[i * span : (i + 1) * span]

    def row_send(j, carry):
        to = lax.rem(row + j, rows)
        remote(r.pay.at[to], r.row_in.at[row], r.sent.at[0], r.p1, target(nx, z, to, y))
        return carry

    lax.fori_loop(1, rows, row_send, 0)
    out_part(y_far)
    over_x(y_left)
    over_x(y_right)
    r.row_in[row] = r.pay[row]

    settle(r.row_in.at[pl.ds(0, rows - 1)], r.p1)
    pull = jnp.zeros((span, 128), F32)
    for j in reversed(range(rows)):
        r.row_out[j] = pull
        pull = pull * jnp.exp(kept_row(j)) + r.row_in[j]
    r.z_out[...] = pull
    r.z_in[z] = pull

    def z_send(j, carry):
        to = lax.rem(z + j, nz)
        remote(r.z_out, r.z_in.at[z], r.sent.at[1], r.p2, target(nx, to, row, y))
        return carry

    lax.fori_loop(1, nz, z_send, 0)
    over_x(y_far)
    inside(r, blocks)

    for q in range(NY):
        over_z(q)

    def last_send(j, carry):
        to = lax.rem(z + j, nz)
        remote(r.last_out.at[to], r.last_in.at[z], r.sent.at[5], r.g3, (to, x, c, y))
        return carry

    lax.fori_loop(1, nz, last_send, 0)

    settle(r.z_in.at[pl.ds(0, nz - 1)], r.p2)
    pull = jnp.zeros((span, 128), F32)
    mine = jnp.zeros((span, 128), F32)
    for k in reversed(range(nz)):
        mine = jnp.where(z == k, pull, mine)
        pull = pull * jnp.exp(kept_z(k)) + r.z_in[k]
    behind = jnp.zeros((1, 128), F32)
    for j in reversed(range(rows)):
        r.row_out[j] = r.row_out[j] + mine * jnp.exp(behind)
        behind = behind + kept_row(j)

    def row_back(j, carry):
        to = lax.rem(row + j, rows)
        remote(r.row_out.at[to], r.ex.at[row], r.sent.at[2], r.p3, target(nx, z, to, y))
        return carry

    lax.fori_loop(1, rows, row_back, 0)
    r.ex[row] = r.row_out[row]

    settle(r.f_ex.at[pl.ds(0, rows - 1)], r.f3)
    settle(r.ex.at[pl.ds(0, rows - 1)], r.p3)
    across(r, blocks, rows, same)

    settle(r.last_in.at[pl.ds(0, nz - 1)], r.g3)
    total = r.last_out[z].astype(F32)
    for j in range(1, nz):
        total = total + r.last_in[lax.rem(z + j, nz)].astype(F32)
    r.gout[...] = total

    settle(r.send.at[pl.ds(0, len(ringed) * rows - 1)], r.send_sem)
    settle(r.full, r.full_sem)
    settle(r.rows.at[pl.ds(0, 3), pl.ds(0, len(ringed) * rows)], r.ring_sem)
    settle(r.part.at[pl.ds(0, 3)], r.back_sem)
    settle(r.ret.at[pl.ds(0, nz * rows - 1)], r.home_sem)
    settle(r.tg.at[pl.ds(0, 3)], r.tg_sem)
    settle(r.pay.at[pl.ds(0, rows - 1)], r.sent.at[0])
    settle(r.z_in.at[pl.ds(0, nz - 1)], r.sent.at[1])
    settle(r.ex.at[pl.ds(0, rows - 1)], r.sent.at[2])
    settle(r.f_pay.at[pl.ds(0, rows - 1)], r.f_sent.at[0])
    settle(r.f_z_in.at[pl.ds(0, nz - 1)], r.f_sent.at[1])
    settle(r.f_ex.at[pl.ds(0, rows - 1)], r.f_sent.at[2])
    settle(r.core_in, r.core_sem)
    settle(r.last_in.at[pl.ds(0, nz - 1)], r.sent.at[5])
    if nx > 1:
        settle(r.x_in.at[:, pl.ds(0, nx - 1)], r.x_sem)


def inside(r, blocks):
    head0 = lax.broadcasted_iota(jnp.int32, (BLOCK, 128), 1) < 64
    le = triangle("le")
    ge = triangle("ge").astype(BF16)
    for b in range(blocks):
        at = slice(b * BLOCK, (b + 1) * BLOCK)
        cum = r.cum[at, :]
        middle = cum[BLOCK // 2 - 1 : BLOCK // 2, :]
        up, down = jnp.exp(cum - middle), jnp.exp(middle - cum)
        q_mid = (r.q[at, :].astype(F32) * 0.125 * up).astype(BF16)
        k_mid = (r.k[at, :].astype(F32) * down).astype(BF16)
        nothing = jnp.zeros_like(q_mid)
        dq_mid = jnp.zeros((BLOCK, 128), F32)
        dk_mid = jnp.zeros((BLOCK, 128), F32)
        for h in range(2):
            cols = slice(h * 128, (h + 1) * 128)
            mine = head0 if h == 0 else jnp.logical_not(head0)
            q_one = jnp.where(mine, q_mid, nothing)
            k_one = jnp.where(mine, k_mid, nothing)
            cot = r.dmix[at, cols]
            scores = jnp.where(le, dot(q_one, k_one, 1, 1), 0.0).astype(BF16)
            d_scores = jnp.where(le, dot(cot, r.v[at, cols], 1, 1), 0.0).astype(BF16)
            dq_mid = dq_mid + dot(d_scores, k_one, 1, 0)
            dk_mid = dk_mid + dot(d_scores, q_one, 0, 0)
            r.dv_in[at, cols] = dot(scores, cot, 0, 0)
        r.dq_in[at, :] = dq_mid * up
        r.dk_in[at, :] = dk_mid * down
        r.dl_in[at, :] = spread_sum(ge, q_mid.astype(F32) * dq_mid - k_mid.astype(F32) * dk_mid)


def across(r, blocks, rows, same):
    ge = triangle("ge").astype(BF16)
    lt = triangle("lt").astype(BF16)

    def opened(ref):
        compact = jnp.concatenate([ref[i] for i in range(rows)], axis=0)
        return jnp.where(same, jnp.concatenate([compact, compact], axis=0), 0.0)

    def end_of(b):
        return jnp.exp(r.cum[(b + 1) * BLOCK - 1 : (b + 1) * BLOCK, :])

    states = [opened(r.f_ex)]
    for b in range(blocks - 1):
        states.append(states[-1] * end_of(b) + r.added[b])
    pulls = [opened(r.ex)]
    for b in reversed(range(1, blocks)):
        pulls.insert(0, pulls[0] * end_of(b) + r.pulled[b])
    for b in range(blocks):
        at = slice(b * BLOCK, (b + 1) * BLOCK)
        cum = r.cum[at, :]
        end = cum[BLOCK - 1 : BLOCK, :]
        query = r.q[at, :].astype(F32) * 0.125
        key = r.k[at, :].astype(F32)
        asked, kept = jnp.exp(cum), jnp.exp(end - cum)
        pull = pulls[b].astype(BF16)
        far_v = dot((key * kept).astype(BF16), pull, 1, 1)
        r.dv[at, :] = (r.dv_in[at, :] + far_v).astype(BF16)
        dq_far = dot(r.dmix[at, :], states[b].astype(BF16), 1, 0) * asked
        dk_far = dot(r.v[at, :], pull, 1, 0) * kept
        r.dq[at, :] = ((r.dq_in[at, :] + dq_far) * 0.125).astype(BF16)
        r.dk[at, :] = (r.dk_in[at, :] + dk_far).astype(BF16)
        carried = jnp.sum(states[b] * pulls[b], axis=0, keepdims=True) * jnp.exp(end)
        r.dl[at, :] = (
            r.dl_in[at, :] + spread_sum(ge, query * dq_far) + spread_sum(lt, key * dk_far) + carried
        )


class Refs:
    pass


def mega(ids, weights, moe, cot, gate, up, down, out_weight, mix, query, key, value, log_decay):
    nz, nx = sizes()
    rows = 2 * nx
    half = rows // 2
    tok, width = moe.shape
    quarter = width // NY
    experts = nz * rows
    per = 2 * tok // experts
    span = 128 // rows
    deep = span + 8
    per_sp = width // experts
    units = gate.shape[1]
    sem = pltpu.SemaphoreType.DMA

    def vm(*shape, dtype=BF16):
        return pltpu.VMEM(shape, dtype)

    ins = [
        "ids_hbm",
        "weights_hbm",
        "moe_hbm",
        "cot_hbm",
        "gate_hbm",
        "up_hbm",
        "down_hbm",
        "ow_hbm",
        "mix_hbm",
        "q_hbm",
        "k_hbm",
        "v_hbm",
        "ld_hbm",
    ]
    outs = {
        "g_gate": (gate.shape, BF16),
        "g_up": (up.shape, BF16),
        "g_down": (down.shape, BF16),
        "gout": ((per_sp, 256), F32),
        "dq": ((tok, 128), BF16),
        "dk": ((tok, 128), BF16),
        "dv": ((tok, 256), BF16),
        "dl": ((tok, 128), F32),
    }
    scratch = {
        "ids": vm(2, tok, dtype=jnp.int32),
        "weights": vm(2, tok, dtype=F32),
        "moe_q": vm(tok, quarter),
        "cot_q": vm(tok, quarter),
        "ld": vm(tok, 128, dtype=F32),
        "k": vm(tok, 128),
        "v": vm(tok, 256),
        "q": vm(tok, 128),
        "gate": vm(*gate.shape),
        "up": vm(*up.shape),
        "down": vm(*down.shape),
        "ow": vm(*out_weight.shape),
        "mix": vm(*mix.shape),
        "pick": vm(2 * tok, tok),
        "send": vm(experts, per, 2 * quarter),
        "rows": vm(NY, experts, per, 2 * quarter),
        "hidden": vm(2 * tok, units),
        "d_gate": vm(2 * tok, units),
        "d_up": vm(2 * tok, units),
        "part": vm(NY, experts, per, quarter),
        "near_l": vm(nz, half, per, quarter),
        "near_r": vm(nz, half, per, quarter),
        "sum_l": vm(nz, half, per, quarter),
        "sum_r": vm(nz, half, per, quarter),
        "last_l": vm(nz, rows, per, quarter),
        "last_r": vm(nz, rows, per, quarter),
        "done": vm(nz, rows, per, quarter),
        "ret": vm(experts, per, quarter),
        "tg": vm(NY, 4, tok // 4, quarter),
        "dmix": vm(tok, 256),
        "cum": vm(tok, 128, dtype=F32),
        "added": vm(tok // BLOCK, 256, 128, dtype=F32),
        "pulled": vm(tok // BLOCK, 256, 128, dtype=F32),
        "dv_in": vm(tok, 256, dtype=F32),
        "dq_in": vm(tok, 128, dtype=F32),
        "dk_in": vm(tok, 128, dtype=F32),
        "dl_in": vm(tok, 128, dtype=F32),
        "moe": vm(tok, width),
        "cot": vm(tok, width),
        "slot_weight": vm(2 * tok, 128, dtype=F32),
        "full": vm(len(FULL.get(nz, (1,))) * rows, NY, per, 2 * quarter),
        "gw": vm(NY, 2, nx, nz // NY, per_sp, 256),
        "f_pay": vm(rows, deep, 128, dtype=F32),
        "f_row_in": vm(rows, deep, 128, dtype=F32),
        "f_z_out": vm(deep, 128, dtype=F32),
        "f_z_in": vm(nz, deep, 128, dtype=F32),
        "f_row_out": vm(rows, span, 128, dtype=F32),
        "f_ex": vm(rows, span, 128, dtype=F32),
        "pay": vm(rows, span, 128, dtype=F32),
        "row_in": vm(rows, span, 128, dtype=F32),
        "z_out": vm(span, 128, dtype=F32),
        "z_in": vm(nz, span, 128, dtype=F32),
        "row_out": vm(rows, span, 128, dtype=F32),
        "ex": vm(rows, span, 128, dtype=F32),
        "core_in": vm(NY, nx, nz // NY, per_sp, 256),
        "x_out": vm(NY, nx, nz // NY, per_sp, 256),
        "x_in": vm(NY, nx, nz // NY, per_sp, 256),
        "last_out": vm(nz, per_sp, 256),
        "last_in": vm(nz, per_sp, 256),
        "ends": vm(rows, 128, dtype=F32),
        "load_sem": sem((15,)),
        "own_sem": sem((2,)),
        "sent": sem((6,)),
        "f_sent": sem((3,)),
    }
    for name in ("send_sem", "ring_sem", "back_sem", "home_sem", "ret_sem", "tg_sem", "p1", "p2", "p3", "g3", "full_sem", "core_sem", "x_sem", "f1", "f2", "f3"):
        scratch[name] = sem
    for name in ("come", "from_l", "from_r", "far_l", "far_r", "a_l", "a_r", "b_l", "b_r"):
        scratch[name] = sem((nz,))
    for name in ("t_l", "t_r", "u_l", "u_r", "g1", "g2"):
        scratch[name] = sem((4,))
    names = ins + list(outs) + list(scratch)

    def body(*refs):
        r = Refs()
        for name, ref in zip(names, refs):
            setattr(r, name, ref)
        mega_kernel(r, nz, nx)

    return pl.pallas_call(
        body,
        name="mega",
        out_shape=tuple(pltpu.VMEM(*kind) for kind in outs.values()),
        in_specs=[pl.BlockSpec(memory_space=pltpu.HBM)] * 13,
        out_specs=(VMEM,) * 8,
        scratch_shapes=list(scratch.values()),
        compiler_params=params(1),
    )(ids, weights, moe, cot, gate, up, down, out_weight, mix, query, key, value, log_decay)


def finish_kernel(*refs):
    count = (len(refs) - 1) // 2
    sem = refs[-1]
    copies = [
        pltpu.make_async_copy(refs[i], refs[count + i], sem.at[i]) for i in range(count)
    ]
    for copy in copies:
        copy.start()
    for copy in copies:
        copy.wait()


def finish(arrays):
    shapes = tuple(jax.ShapeDtypeStruct(a.shape, a.dtype) for a in arrays)
    return pl.pallas_call(
        finish_kernel,
        name="finish",
        out_shape=shapes,
        in_specs=[VMEM] * len(arrays),
        out_specs=(ANY,) * len(arrays),
        scratch_shapes=[pltpu.SemaphoreType.DMA((len(arrays),))],
        compiler_params=pltpu.CompilerParams(vmem_limit_bytes=1024 * 1024),
    )(*[pltpu.with_memory_space_constraint(a, pltpu.VMEM) for a in arrays])


def shards(
    moe_input,
    cotangent,
    expert_ids,
    route_weights,
    gate_weight,
    up_weight,
    down_weight,
    out_weight,
    mixer_out,
    query_vectors,
    key_vectors,
    value_vectors,
    log_decay,
):
    results = mega(
        expert_ids.T,
        route_weights.T,
        moe_input,
        cotangent,
        gate_weight[0],
        up_weight[0],
        down_weight[0],
        out_weight,
        mixer_out,
        query_vectors,
        key_vectors,
        value_vectors,
        log_decay,
    )
    g_gate, g_up, g_down, gout, dq, dk, dv, dl = finish(results)
    return g_gate[None], g_up[None], g_down[None], gout, dq, dk, dv, dl


def solution(mesh):
    finer = Mesh(mesh.devices.reshape(8, 4, 2, mesh.shape["tp"]), ("sp_0", "sp_1", "sp_2", "tp"))
    in_specs = (
        P(SP, None),
        P(SP, None),
        P(SP, None),
        P(SP, None),
        P(SP, None, "tp"),
        P(SP, None, "tp"),
        P(SP, "tp", None),
        P(None, "tp"),
        P(SP, "tp"),
        P(SP, "tp"),
        P(SP, "tp"),
        P(SP, "tp"),
        P(SP, "tp"),
    )
    out_specs = (
        P(SP, None, "tp"),
        P(SP, None, "tp"),
        P(SP, "tp", None),
        P(SP, "tp"),
        P(SP, "tp"),
        P(SP, "tp"),
        P(SP, "tp"),
        P(SP, "tp"),
    )
    return jax.shard_map(
        shards, mesh=finer, in_specs=in_specs, out_specs=out_specs, check_vma=False
    )
```

```python
import jax
import jax.numpy as jnp
from jax import lax
from jax.experimental import pallas as pl
from jax.experimental.pallas import tpu as pltpu
from jax.sharding import Mesh
from jax.sharding import PartitionSpec as P

MESH = pl.DeviceIdType.MESH
SP = ("sp_0", "sp_1", "sp_2")
BF16 = jnp.bfloat16
F32 = jnp.float32
NY = 4
FULL = {8: (5, 7)}
ORDER = {8: (0, 2, 6, 3, 5, 1, 4, 7)}
BLOCK = 64
VMEM = pl.BlockSpec(memory_space=pltpu.VMEM)
ANY = pl.BlockSpec(memory_space=pl.ANY)


def sizes():
    return lax.axis_size("sp_0"), lax.axis_size("sp_1")


def params(collective_id=None):
    if collective_id is None:
        return pltpu.CompilerParams(vmem_limit_bytes=60 * 1024 * 1024)
    return pltpu.CompilerParams(
        collective_id=collective_id, has_side_effects=True, vmem_limit_bytes=60 * 1024 * 1024
    )


def dot(a, b, ca, cb):
    return lax.dot_general(a, b, (((ca,), (cb,)), ((), ())), preferred_element_type=F32)


def place():
    return (
        lax.axis_index("sp_0"),
        lax.axis_index("sp_1"),
        lax.axis_index("sp_2"),
        lax.axis_index("tp"),
    )


def target(nx, zz, row, y):
    return (zz, row // 2, row % 2, y)


def offset(k, nz):
    order = ORDER.get(nz, tuple(range(nz)))
    out = 0
    for i, ahead in enumerate(order):
        out = out + jnp.where(k == i, ahead, 0)
    return out


def settle(ref, sem):
    pltpu.make_async_copy(ref, ref, sem).wait()


def greet_plane(barrier, nz, nx, z, x, c, y):
    def hello(device):
        pl.semaphore_signal(barrier, inc=1, device_id=device, device_id_type=MESH)

    columns = [lax.rem(x + i, nx) for i in range(nx)]

    def level(zz, own):
        for i in reversed(range(nx)):
            hello((zz, columns[i], 1 - c, y))
            if i or not own:
                hello((zz, columns[i], c, y))

    def level_at(i, carry):
        away = jnp.where(i % 2 == 0, nz // 2 - i // 2, nz // 2 + 1 + i // 2)
        level(lax.rem(z + away, nz), False)
        return carry

    lax.fori_loop(0, nz - 1, level_at, 0)
    level(z, True)
    for side in (1, NY - 1):
        hello((z, x, c, lax.rem(y + side, NY)))


def remote(src, dst, send_sem, recv_sem, device):
    copy = pltpu.make_async_remote_copy(
        src_ref=src,
        dst_ref=dst,
        send_sem=send_sem,
        recv_sem=recv_sem,
        device_id=device,
        device_id_type=MESH,
    )
    copy.start()


def triangle(kind):
    row = lax.broadcasted_iota(jnp.int32, (BLOCK, BLOCK), 0)
    col = lax.broadcasted_iota(jnp.int32, (BLOCK, BLOCK), 1)
    return {"le": col <= row, "ge": col >= row, "lt": col < row}[kind]


def spread_sum(tri, value):
    high = value.astype(BF16)
    rest = value - high.astype(F32)
    mid = rest.astype(BF16)
    low = (rest - mid.astype(F32)).astype(BF16)
    both = jnp.concatenate([high, mid, low], axis=0)
    return dot(jnp.concatenate([tri, tri, tri], axis=1), both, 1, 0)


def diagonal(shape):
    return (lax.broadcasted_iota(jnp.int32, shape, 0) < shape[0] // 2) == (
        lax.broadcasted_iota(jnp.int32, shape, 1) < shape[1] // 2
    )


def mega_kernel(r, nz, nx):
    z, x, c, y = place()
    rows = 2 * nx
    row = x * 2 + c
    me = z * rows + row
    half = rows // 2
    tok, quarter = r.moe_q.shape
    experts, per = nz * rows, 2 * tok // (nz * rows)
    slots = 2 * tok
    units = r.gate.shape[1]
    y_left, y_right = lax.rem(y + NY - 1, NY), lax.rem(y + 1, NY)
    y_far = lax.rem(y + 2, NY)
    right = target(nx, z, row, y_right)
    left = target(nx, z, row, y_left)
    cols = pl.ds(pl.multiple_of(y * quarter, quarter), quarter)
    loads = [
        pltpu.make_async_copy(src, dst, r.load_sem.at[i])
        for i, (src, dst) in enumerate(
            (
                (r.ids_hbm, r.ids),
                (r.weights_hbm, r.weights),
                (r.moe_hbm.at[:, cols], r.moe_q),
                (r.cot_hbm.at[:, cols], r.cot_q),
                (r.ld_hbm, r.ld),
                (r.k_hbm, r.k),
                (r.v_hbm, r.v),
                (r.gate_hbm, r.gate),
                (r.up_hbm, r.up),
                (r.down_hbm, r.down),
                (r.q_hbm, r.q),
                (r.ow_hbm, r.ow),
                (r.mix_hbm, r.mix),
                (r.moe_hbm, r.moe),
                (r.cot_hbm, r.cot),
            )
        )
    ]
    for load in loads[:4]:
        load.start()
    barrier = pltpu.get_barrier_semaphore()
    greet_plane(barrier, nz, nx, z, x, c, y)

    for load in loads[4:]:
        load.start()
    for load in loads[:2]:
        load.wait()
    lanes = max(128, experts)
    which = lax.broadcasted_iota(jnp.int32, (lanes, tok), 0)
    hot = [(r.ids[j : j + 1, :] == which).astype(F32) for j in range(2)]
    earlier = (
        lax.broadcasted_iota(jnp.int32, (tok, tok), 0)
        < lax.broadcasted_iota(jnp.int32, (tok, tok), 1)
    ).astype(BF16)
    before = dot((hot[0] + hot[1]).astype(BF16), earlier, 1, 0)
    slot_iota = lax.broadcasted_iota(jnp.int32, (slots, tok), 0)
    picks = []
    for j in range(2):
        rank = jnp.sum(before * hot[j], axis=0, keepdims=True).astype(jnp.int32)
        slot = r.ids[j : j + 1, :] * per + rank
        picks.append((slot == slot_iota).astype(BF16))
    both = picks[0] + picks[1]
    r.pick[...] = both
    slot_weight = jnp.zeros((slots, 1), F32)
    for j in range(2):
        chosen = picks[j].astype(F32) * r.weights[j : j + 1, :]
        slot_weight = slot_weight + jnp.sum(chosen, axis=1, keepdims=True)
    r.slot_weight[...] = jnp.broadcast_to(slot_weight, (slots, 128))
    loads[2].wait()
    sorted_rows = dot(both, r.moe_q[...], 1, 0).astype(BF16)
    r.send[:, :, 0:quarter] = sorted_rows.reshape(experts, per, quarter)
    loads[3].wait()
    sorted_cot = (dot(both, r.cot_q[...], 1, 0) * slot_weight).astype(BF16)
    r.send[:, :, quarter:] = sorted_cot.reshape(experts, per, quarter)
    pl.semaphore_wait(barrier, nz * rows + 1)

    def scatter(i, carry):
        k, j = i // rows, lax.rem(i, rows)
        zz = lax.rem(z - offset(k, nz) + nz, nz)
        to = lax.rem(row + j, rows)
        remote(
            r.send.at[zz * rows + to],
            r.rows.at[y, k * rows + row],
            r.send_sem,
            r.come.at[k],
            target(nx, zz, to, y),
        )
        return carry

    own = pltpu.make_async_copy(r.send.at[me], r.rows.at[y, row], r.own_sem.at[0])
    own.start()
    wide = FULL.get(nz, (nz - 1,))
    ringed = [k for k in range(nz) if k not in wide]
    lines = rows * per

    def fill(i, k):
        zz = lax.rem(z - offset(k, nz) + nz, nz)
        there = pl.ds(pl.multiple_of(zz * lines, lines), lines)
        pick_there = r.pick[there, :]
        weight_there = r.slot_weight[there, 0:1]
        block = slice(i * rows, (i + 1) * rows)
        for q in range(NY):
            part = slice(q * quarter, (q + 1) * quarter)
            value = dot(pick_there, r.moe[:, part], 1, 0).astype(BF16)
            r.full[block, q, :, 0:quarter] = value.reshape(rows, per, quarter)
            value = (dot(pick_there, r.cot[:, part], 1, 0) * weight_there).astype(BF16)
            r.full[block, q, :, quarter:] = value.reshape(rows, per, quarter)

    def scatter_full(i, k):
        zz = lax.rem(z - offset(k, nz) + nz, nz)

        def one(j, carry):
            to = lax.rem(row + j, rows)
            remote(
                r.full.at[i * rows + to],
                r.rows.at[:, k * rows + row],
                r.full_sem,
                r.come.at[k],
                target(nx, zz, to, y),
            )
            return carry

        lax.fori_loop(0, rows, one, 0)

    begin = 1
    for i, k in enumerate(wide):
        lax.fori_loop(begin, k * rows, scatter, 0)
        if i == 0:
            loads[13].wait()
            loads[14].wait()
            for ii, kk in enumerate(wide):
                fill(ii, kk)
        scatter_full(i, k)
        begin = (k + 1) * rows
    if begin < nz * rows:
        lax.fori_loop(begin, nz * rows, scatter, 0)
    own.wait()

    def is_ring(k):
        answer = k >= 0
        for w in wide:
            answer = answer & (k != w)
        return answer

    blocks = tok // BLOCK
    same = diagonal((256, 128))
    tri = triangle("le").astype(BF16)
    for load in loads[4:7]:
        load.wait()
    state = jnp.zeros((256, 128), F32)
    for b in range(blocks):
        at = slice(b * BLOCK, (b + 1) * BLOCK)
        cum = spread_sum(tri, r.ld[at, :])
        r.cum[at, :] = cum
        end = cum[BLOCK - 1 : BLOCK, :]
        kept = (r.k[at, :].astype(F32) * jnp.exp(end - cum)).astype(BF16)
        added = jnp.where(same, dot(r.v[at, :], kept, 0, 0), 0.0)
        r.added[b] = added
        state = state * jnp.exp(end) + added
        whole = end if b == 0 else whole + end
    state = state[0:128] + state[128:256]
    span = 128 // rows
    for i in range(rows):
        r.f_pay[i, 0:span, :] = state[i * span : (i + 1) * span]
        r.f_pay[i, span:, :] = jnp.broadcast_to(whole, (8, 128))

    def f_send(j, carry):
        to = lax.rem(row + j, rows)
        remote(r.f_pay.at[to], r.f_row_in.at[row], r.f_sent.at[0], r.f1, target(nx, z, to, y))
        return carry

    lax.fori_loop(1, rows, f_send, 0)
    r.f_row_in[row] = r.f_pay[row]

    def kept_row(j):
        return r.f_row_in[j, span : span + 1, :]

    def kept_z(k):
        return r.f_z_in[k, span : span + 1, :]

    def forward_row():
        settle(r.f_row_in.at[pl.ds(0, rows - 1)], r.f1)
        state = jnp.zeros((span, 128), F32)
        after = jnp.zeros((1, 128), F32)
        for j in range(rows):
            r.f_row_out[j] = state
            r.ends[j : j + 1, :] = after
            state = state * jnp.exp(kept_row(j)) + r.f_row_in[j, 0:span, :]
            after = after + kept_row(j)
        r.f_z_out[0:span, :] = state
        r.f_z_out[span:, :] = jnp.broadcast_to(after, (8, 128))
        r.f_z_in[z] = r.f_z_out[...]

        def send(j, carry):
            to = lax.rem(z + j, nz)
            remote(r.f_z_out, r.f_z_in.at[z], r.f_sent.at[1], r.f2, target(nx, to, row, y))
            return carry

        lax.fori_loop(1, nz, send, 0)

    def forward_z():
        settle(r.f_z_in.at[pl.ds(0, nz - 1)], r.f2)
        state = jnp.zeros((span, 128), F32)
        mine = jnp.zeros((span, 128), F32)
        for k in range(nz):
            mine = jnp.where(z == k, state, mine)
            state = state * jnp.exp(kept_z(k)) + r.f_z_in[k, 0:span, :]
        for j in range(rows):
            r.f_row_out[j] = r.f_row_out[j] + mine * jnp.exp(r.ends[j : j + 1, :])

        def send(j, carry):
            to = lax.rem(row + j, rows)
            remote(r.f_row_out.at[to], r.f_ex.at[row], r.f_sent.at[2], r.f3, target(nx, z, to, y))
            return carry

        lax.fori_loop(1, rows, send, 0)
        r.f_ex[row] = r.f_row_out[row]

    for load in loads[7:13]:
        load.wait()

    def chunk(k):
        return pl.ds(k * rows, rows)

    def spread(k):
        block = r.rows.at[y, chunk(k)]
        remote(block, block, r.ring_sem, r.from_l.at[k], right)
        remote(block, block, r.ring_sem, r.from_r.at[k], left)

    def onward(k):
        settle(r.rows.at[y_left, chunk(k)], r.from_l.at[k])
        block = r.rows.at[y_left, pl.ds(k * rows, half)]
        remote(block, block, r.ring_sem, r.far_l.at[k], right)
        settle(r.rows.at[y_right, chunk(k)], r.from_r.at[k])
        block = r.rows.at[y_right, pl.ds(k * rows + half, half)]
        remote(block, block, r.ring_sem, r.far_r.at[k], left)

    def gathered(k):
        settle(r.rows.at[y, pl.ds(0, half)], r.far_l.at[k])
        settle(r.rows.at[y, pl.ds(0, half)], r.far_r.at[k])

    def expert(k):
        pre_gate = jnp.zeros((lines, units), F32)
        pre_up = jnp.zeros((lines, units), F32)
        delta = jnp.zeros((lines, units), F32)
        for q in range(NY):
            part = slice(q * quarter, (q + 1) * quarter)
            routed = r.rows[q, chunk(k), :, 0:quarter].reshape(lines, quarter)
            routed_cot = r.rows[q, chunk(k), :, quarter:].reshape(lines, quarter)
            pre_gate = pre_gate + dot(routed, r.gate[part, :], 1, 0)
            pre_up = pre_up + dot(routed, r.up[part, :], 1, 0)
            delta = delta + dot(routed_cot, r.down[:, part], 1, 1)
        sig = jax.nn.sigmoid(pre_gate)
        act = pre_gate * sig
        d_gate = (delta * pre_up * sig * (1.0 + pre_gate * (1.0 - sig))).astype(BF16)
        d_up = (delta * act).astype(BF16)
        at = pl.ds(pl.multiple_of(k * lines, lines), lines)
        r.hidden[at, :] = (act * pre_up).astype(BF16)
        r.d_gate[at, :] = d_gate
        r.d_up[at, :] = d_up

        def give(i, carry):
            q = lax.rem(y + 2 + i, NY)
            part = pl.ds(pl.multiple_of(q * quarter, quarter), quarter)
            value = dot(d_gate, r.gate[part, :], 1, 1) + dot(d_up, r.up[part, :], 1, 1)
            r.part[q, chunk(k)] = value.astype(BF16).reshape(rows, per, quarter)
            return carry

        give(0, 0)
        remote(
            r.part.at[y_far, pl.ds(k * rows, half)],
            r.near_l.at[k], r.back_sem, r.a_l.at[k], right,
        )
        remote(
            r.part.at[y_far, pl.ds(k * rows + half, half)],
            r.near_r.at[k], r.back_sem, r.a_r.at[k], left,
        )
        lax.fori_loop(1, NY, give, 0)
        remote(
            r.part.at[y_right, pl.ds(k * rows + half, half)],
            r.last_l.at[k, pl.ds(half, half)], r.back_sem, r.b_l.at[k], right,
        )
        remote(
            r.part.at[y_left, pl.ds(k * rows, half)],
            r.last_r.at[k, pl.ds(0, half)], r.back_sem, r.b_r.at[k], left,
        )

    def second(k):
        settle(r.near_l.at[k], r.a_l.at[k])
        r.sum_r[k] = (
            r.part[y_right, pl.ds(k * rows, half)].astype(F32) + r.near_l[k].astype(F32)
        ).astype(BF16)
        remote(r.sum_r.at[k], r.last_l.at[k, pl.ds(0, half)], r.back_sem, r.b_l.at[k], right)
        settle(r.near_r.at[k], r.a_r.at[k])
        r.sum_l[k] = (
            r.part[y_left, pl.ds(k * rows + half, half)].astype(F32) + r.near_r[k].astype(F32)
        ).astype(BF16)
        remote(r.sum_l.at[k], r.last_r.at[k, pl.ds(half, half)], r.back_sem, r.b_r.at[k], left)

    def third(k, begin):
        settle(r.last_l.at[k], r.b_l.at[k])
        settle(r.last_r.at[k], r.b_r.at[k])
        r.done[k] = (
            r.part[y, chunk(k)].astype(F32)
            + r.last_l[k].astype(F32)
            + r.last_r[k].astype(F32)
        ).astype(BF16)
        zz = lax.rem(z + offset(k, nz) + nz, nz)

        def home(j, carry):
            to = lax.rem(row + j, rows)
            remote(r.done.at[k, to], r.ret.at[me], r.home_sem, r.ret_sem, target(nx, zz, to, y))
            return carry

        lax.fori_loop(begin, rows, home, 0)

    def arrive(k):
        settle(r.rows.at[y, pl.ds(0, rows)], r.come.at[k])
        spread(k)

    settle(r.rows.at[y, pl.ds(0, rows - 1)], r.come.at[0])
    spread(0)
    arrive(1)
    onward(0)

    def step(t, carry):
        @pl.when(is_ring(t + 1) & (t + 1 < nz))
        def _():
            arrive(t + 1)

        @pl.when(is_ring(t) & (t < nz))
        def _():
            onward(t)

        @pl.when(is_ring(t - 1))
        def _():
            gathered(t - 1)

        @pl.when(jnp.logical_not(is_ring(t - 1)))
        def _():
            settle(r.rows.at[0, pl.ds(0, NY * rows)], r.come.at[t - 1])

        expert(t - 1)

        @pl.when(t >= 2)
        def _():
            second(t - 2)

        @pl.when(t == 2)
        def _():
            forward_row()

        @pl.when(t == nz // 2 + 1)
        def _():
            forward_z()

        @pl.when(t == 3)
        def _():
            third(0, 1)
            home = pltpu.make_async_copy(r.done.at[0, row], r.ret.at[me], r.own_sem.at[1])
            home.start()
            home.wait()

        @pl.when(t >= 4)
        def _():
            third(t - 3, 0)

        return carry

    lax.fori_loop(1, nz + 1, step, 0)

    def routed_of(q, lower):
        return r.rows[q, :, :, lower : lower + quarter].reshape(slots, quarter)

    def grads(kind, q):
        part = slice(q * quarter, (q + 1) * quarter)
        if kind == "down":
            r.g_down[:, part] = dot(r.hidden[...], routed_of(q, quarter), 0, 0).astype(BF16)
        else:
            routed = routed_of(q, 0)
            r.g_gate[part, :] = dot(routed, r.d_gate[...], 0, 0).astype(BF16)
            r.g_up[part, :] = dot(routed, r.d_up[...], 0, 0).astype(BF16)

    grads("down", 0)
    grads("down", 1)
    second(nz - 1)
    third(nz - 2, 0)
    grads("down", 2)
    grads("down", 3)
    third(nz - 1, 0)
    for q in range(NY):
        grads("both", q)
    settle(r.ret.at[pl.ds(0, nz * rows - 1)], r.ret_sem)

    pieces, length = r.tg.shape[1], r.tg.shape[2]
    mid = length // 2
    returned = r.ret[...].reshape(slots, quarter)
    for i in range(pieces):
        at = slice(i * length, (i + 1) * length)
        sums = dot(r.pick[:, at], returned, 0, 0)
        r.tg[y, i] = (r.cot_q[at, :].astype(F32) + sums).astype(BF16)
        block = r.tg.at[y, i]
        remote(block, block, r.tg_sem, r.t_l.at[i], right)
        remote(block, block, r.tg_sem, r.t_r.at[i], left)

    per_sp = r.gw.shape[4]
    deep_z = r.gw.shape[3]
    many = quarter // per_sp

    def mixed(q):
        return dot(
            r.tg[q].reshape(tok, quarter),
            r.ow[pl.ds(pl.multiple_of(q * quarter, quarter), quarter), :], 1, 0,
        )

    def out_part(q):
        grad = dot(r.tg[q].reshape(tok, quarter), r.mix[...], 0, 0).astype(BF16)
        for m in range(many):
            r.gw[q, m % 2, (m // 2) % nx, m // rows] = grad[m * per_sp : (m + 1) * per_sp]
        remote(r.gw.at[q, 1 - c], r.core_in.at[q], r.core_sem, r.g1.at[q], (z, x, 1 - c, y))

    def over_x(q):
        settle(r.core_in.at[q], r.g1.at[q])
        r.x_out[q] = (r.gw[q, c].astype(F32) + r.core_in[q].astype(F32)).astype(BF16)

        def x_send(j, carry):
            to = lax.rem(x + j, nx)
            remote(r.x_out.at[q, to], r.x_in.at[q, x], r.x_sem, r.g2.at[q], (z, to, c, y))
            return carry

        lax.fori_loop(1, nx, x_send, 0)

    def over_z(q):
        if nx > 1:
            settle(r.x_in.at[q, pl.ds(0, nx - 1)], r.g2.at[q])
        total = r.x_out[q, x].astype(F32)
        for j in range(1, nx):
            total = total + r.x_in[q, lax.rem(x + j, nx)].astype(F32)
        r.last_out[pl.ds(q * deep_z, deep_z)] = total.astype(BF16)

    value = mixed(y)
    out_part(y)

    def tg_onward(i, carry):
        settle(r.tg.at[y_left, i], r.t_l.at[i])
        block = r.tg.at[y_left, i, pl.ds(0, mid)]
        remote(block, block, r.tg_sem, r.u_l.at[i], right)
        settle(r.tg.at[y_right, i], r.t_r.at[i])
        block = r.tg.at[y_right, i, pl.ds(mid, mid)]
        remote(block, block, r.tg_sem, r.u_r.at[i], left)
        return carry

    lax.fori_loop(0, pieces, tg_onward, 0)
    value = value + mixed(y_left) + mixed(y_right)
    out_part(y_left)
    out_part(y_right)
    over_x(y)

    def tg_finish(i, carry):
        settle(r.tg.at[y, i, pl.ds(0, mid)], r.u_l.at[i])
        settle(r.tg.at[y, i, pl.ds(0, mid)], r.u_r.at[i])
        return carry

    lax.fori_loop(0, pieces, tg_finish, 0)
    r.dmix[...] = (value + mixed(y_far)).astype(BF16)

    pull = jnp.zeros((256, 128), F32)
    for b in reversed(range(blocks)):
        at = slice(b * BLOCK, (b + 1) * BLOCK)
        cum = r.cum[at, :]
        end = cum[BLOCK - 1 : BLOCK, :]
        asked = (r.q[at, :].astype(F32) * 0.125 * jnp.exp(cum)).astype(BF16)
        pulled = jnp.where(same, dot(r.dmix[at, :], asked, 0, 0), 0.0)
        r.pulled[b] = pulled
        pull = pull * jnp.exp(end) + pulled
    pull = pull[0:128] + pull[128:256]
    for i in range(rows):
        r.pay[i] = pull[i * span : (i + 1) * span]

    def row_send(j, carry):
        to = lax.rem(row + j, rows)
        remote(r.pay.at[to], r.row_in.at[row], r.sent.at[0], r.p1, target(nx, z, to, y))
        return carry

    lax.fori_loop(1, rows, row_send, 0)
    out_part(y_far)
    over_x(y_left)
    over_x(y_right)
    r.row_in[row] = r.pay[row]

    settle(r.row_in.at[pl.ds(0, rows - 1)], r.p1)
    pull = jnp.zeros((span, 128), F32)
    for j in reversed(range(rows)):
        r.row_out[j] = pull
        pull = pull * jnp.exp(kept_row(j)) + r.row_in[j]
    r.z_out[...] = pull
    r.z_in[z] = pull

    def z_send(j, carry):
        to = lax.rem(z + j, nz)
        remote(r.z_out, r.z_in.at[z], r.sent.at[1], r.p2, target(nx, to, row, y))
        return carry

    lax.fori_loop(1, nz, z_send, 0)
    over_x(y_far)
    inside(r, blocks)

    settle(r.z_in.at[pl.ds(0, nz - 1)], r.p2)
    pull = jnp.zeros((span, 128), F32)
    mine = jnp.zeros((span, 128), F32)
    for k in reversed(range(nz)):
        mine = jnp.where(z == k, pull, mine)
        pull = pull * jnp.exp(kept_z(k)) + r.z_in[k]
    behind = jnp.zeros((1, 128), F32)
    for j in reversed(range(rows)):
        r.row_out[j] = r.row_out[j] + mine * jnp.exp(behind)
        behind = behind + kept_row(j)

    def row_back(j, carry):
        to = lax.rem(row + j, rows)
        remote(r.row_out.at[to], r.ex.at[row], r.sent.at[2], r.p3, target(nx, z, to, y))
        return carry

    lax.fori_loop(1, rows, row_back, 0)
    r.ex[row] = r.row_out[row]

    for q in range(NY):
        over_z(q)

    def last_send(j, carry):
        to = lax.rem(z + j, nz)
        remote(r.last_out.at[to], r.last_in.at[z], r.sent.at[5], r.g3, (to, x, c, y))
        return carry

    lax.fori_loop(1, nz, last_send, 0)

    settle(r.f_ex.at[pl.ds(0, rows - 1)], r.f3)
    settle(r.ex.at[pl.ds(0, rows - 1)], r.p3)
    across(r, blocks, rows, same)

    settle(r.last_in.at[pl.ds(0, nz - 1)], r.g3)
    total = r.last_out[z].astype(F32)
    for j in range(1, nz):
        total = total + r.last_in[lax.rem(z + j, nz)].astype(F32)
    r.gout[...] = total

    settle(r.send.at[pl.ds(0, len(ringed) * rows - 1)], r.send_sem)
    settle(r.full, r.full_sem)
    settle(r.rows.at[pl.ds(0, 3), pl.ds(0, len(ringed) * rows)], r.ring_sem)
    settle(r.part.at[pl.ds(0, 3)], r.back_sem)
    settle(r.ret.at[pl.ds(0, nz * rows - 1)], r.home_sem)
    settle(r.tg.at[pl.ds(0, 3)], r.tg_sem)
    settle(r.pay.at[pl.ds(0, rows - 1)], r.sent.at[0])
    settle(r.z_in.at[pl.ds(0, nz - 1)], r.sent.at[1])
    settle(r.ex.at[pl.ds(0, rows - 1)], r.sent.at[2])
    settle(r.f_pay.at[pl.ds(0, rows - 1)], r.f_sent.at[0])
    settle(r.f_z_in.at[pl.ds(0, nz - 1)], r.f_sent.at[1])
    settle(r.f_ex.at[pl.ds(0, rows - 1)], r.f_sent.at[2])
    settle(r.core_in, r.core_sem)
    settle(r.last_in.at[pl.ds(0, nz - 1)], r.sent.at[5])
    if nx > 1:
        settle(r.x_in.at[:, pl.ds(0, nx - 1)], r.x_sem)


def inside(r, blocks):
    head0 = lax.broadcasted_iota(jnp.int32, (BLOCK, 128), 1) < 64
    le = triangle("le")
    ge = triangle("ge").astype(BF16)
    for b in range(blocks):
        at = slice(b * BLOCK, (b + 1) * BLOCK)
        cum = r.cum[at, :]
        middle = cum[BLOCK // 2 - 1 : BLOCK // 2, :]
        up, down = jnp.exp(cum - middle), jnp.exp(middle - cum)
        q_mid = (r.q[at, :].astype(F32) * 0.125 * up).astype(BF16)
        k_mid = (r.k[at, :].astype(F32) * down).astype(BF16)
        nothing = jnp.zeros_like(q_mid)
        dq_mid = jnp.zeros((BLOCK, 128), F32)
        dk_mid = jnp.zeros((BLOCK, 128), F32)
        for h in range(2):
            cols = slice(h * 128, (h + 1) * 128)
            mine = head0 if h == 0 else jnp.logical_not(head0)
            q_one = jnp.where(mine, q_mid, nothing)
            k_one = jnp.where(mine, k_mid, nothing)
            cot = r.dmix[at, cols]
            scores = jnp.where(le, dot(q_one, k_one, 1, 1), 0.0).astype(BF16)
            d_scores = jnp.where(le, dot(cot, r.v[at, cols], 1, 1), 0.0).astype(BF16)
            dq_mid = dq_mid + dot(d_scores, k_one, 1, 0)
            dk_mid = dk_mid + dot(d_scores, q_one, 0, 0)
            r.dv_in[at, cols] = dot(scores, cot, 0, 0)
        r.dq_in[at, :] = dq_mid * up
        r.dk_in[at, :] = dk_mid * down
        r.dl_in[at, :] = spread_sum(ge, q_mid.astype(F32) * dq_mid - k_mid.astype(F32) * dk_mid)


def across(r, blocks, rows, same):
    ge = triangle("ge").astype(BF16)
    lt = triangle("lt").astype(BF16)

    def opened(ref):
        compact = jnp.concatenate([ref[i] for i in range(rows)], axis=0)
        return jnp.where(same, jnp.concatenate([compact, compact], axis=0), 0.0)

    def end_of(b):
        return jnp.exp(r.cum[(b + 1) * BLOCK - 1 : (b + 1) * BLOCK, :])

    states = [opened(r.f_ex)]
    for b in range(blocks - 1):
        states.append(states[-1] * end_of(b) + r.added[b])
    pulls = [opened(r.ex)]
    for b in reversed(range(1, blocks)):
        pulls.insert(0, pulls[0] * end_of(b) + r.pulled[b])
    for b in range(blocks):
        at = slice(b * BLOCK, (b + 1) * BLOCK)
        cum = r.cum[at, :]
        end = cum[BLOCK - 1 : BLOCK, :]
        query = r.q[at, :].astype(F32) * 0.125
        key = r.k[at, :].astype(F32)
        asked, kept = jnp.exp(cum), jnp.exp(end - cum)
        pull = pulls[b].astype(BF16)
        far_v = dot((key * kept).astype(BF16), pull, 1, 1)
        r.dv[at, :] = (r.dv_in[at, :] + far_v).astype(BF16)
        dq_far = dot(r.dmix[at, :], states[b].astype(BF16), 1, 0) * asked
        dk_far = dot(r.v[at, :], pull, 1, 0) * kept
        r.dq[at, :] = ((r.dq_in[at, :] + dq_far) * 0.125).astype(BF16)
        r.dk[at, :] = (r.dk_in[at, :] + dk_far).astype(BF16)
        carried = jnp.sum(states[b] * pulls[b], axis=0, keepdims=True) * jnp.exp(end)
        r.dl[at, :] = (
            r.dl_in[at, :] + spread_sum(ge, query * dq_far) + spread_sum(lt, key * dk_far) + carried
        )


class Refs:
    pass


def mega(ids, weights, moe, cot, gate, up, down, out_weight, mix, query, key, value, log_decay):
    nz, nx = sizes()
    rows = 2 * nx
    half = rows // 2
    tok, width = moe.shape
    quarter = width // NY
    experts = nz * rows
    per = 2 * tok // experts
    span = 128 // rows
    deep = span + 8
    per_sp = width // experts
    units = gate.shape[1]
    sem = pltpu.SemaphoreType.DMA

    def vm(*shape, dtype=BF16):
        return pltpu.VMEM(shape, dtype)

    ins = [
        "ids_hbm",
        "weights_hbm",
        "moe_hbm",
        "cot_hbm",
        "gate_hbm",
        "up_hbm",
        "down_hbm",
        "ow_hbm",
        "mix_hbm",
        "q_hbm",
        "k_hbm",
        "v_hbm",
        "ld_hbm",
    ]
    outs = {
        "g_gate": (gate.shape, BF16),
        "g_up": (up.shape, BF16),
        "g_down": (down.shape, BF16),
        "gout": ((per_sp, 256), F32),
        "dq": ((tok, 128), BF16),
        "dk": ((tok, 128), BF16),
        "dv": ((tok, 256), BF16),
        "dl": ((tok, 128), F32),
    }
    scratch = {
        "ids": vm(2, tok, dtype=jnp.int32),
        "weights": vm(2, tok, dtype=F32),
        "moe_q": vm(tok, quarter),
        "cot_q": vm(tok, quarter),
        "ld": vm(tok, 128, dtype=F32),
        "k": vm(tok, 128),
        "v": vm(tok, 256),
        "q": vm(tok, 128),
        "gate": vm(*gate.shape),
        "up": vm(*up.shape),
        "down": vm(*down.shape),
        "ow": vm(*out_weight.shape),
        "mix": vm(*mix.shape),
        "pick": vm(2 * tok, tok),
        "send": vm(experts, per, 2 * quarter),
        "rows": vm(NY, experts, per, 2 * quarter),
        "hidden": vm(2 * tok, units),
        "d_gate": vm(2 * tok, units),
        "d_up": vm(2 * tok, units),
        "part": vm(NY, experts, per, quarter),
        "near_l": vm(nz, half, per, quarter),
        "near_r": vm(nz, half, per, quarter),
        "sum_l": vm(nz, half, per, quarter),
        "sum_r": vm(nz, half, per, quarter),
        "last_l": vm(nz, rows, per, quarter),
        "last_r": vm(nz, rows, per, quarter),
        "done": vm(nz, rows, per, quarter),
        "ret": vm(experts, per, quarter),
        "tg": vm(NY, 8, tok // 8, quarter),
        "dmix": vm(tok, 256),
        "cum": vm(tok, 128, dtype=F32),
        "added": vm(tok // BLOCK, 256, 128, dtype=F32),
        "pulled": vm(tok // BLOCK, 256, 128, dtype=F32),
        "dv_in": vm(tok, 256, dtype=F32),
        "dq_in": vm(tok, 128, dtype=F32),
        "dk_in": vm(tok, 128, dtype=F32),
        "dl_in": vm(tok, 128, dtype=F32),
        "moe": vm(tok, width),
        "cot": vm(tok, width),
        "slot_weight": vm(2 * tok, 128, dtype=F32),
        "full": vm(len(FULL.get(nz, (1,))) * rows, NY, per, 2 * quarter),
        "gw": vm(NY, 2, nx, nz // NY, per_sp, 256),
        "f_pay": vm(rows, deep, 128, dtype=F32),
        "f_row_in": vm(rows, deep, 128, dtype=F32),
        "f_z_out": vm(deep, 128, dtype=F32),
        "f_z_in": vm(nz, deep, 128, dtype=F32),
        "f_row_out": vm(rows, span, 128, dtype=F32),
        "f_ex": vm(rows, span, 128, dtype=F32),
        "pay": vm(rows, span, 128, dtype=F32),
        "row_in": vm(rows, span, 128, dtype=F32),
        "z_out": vm(span, 128, dtype=F32),
        "z_in": vm(nz, span, 128, dtype=F32),
        "row_out": vm(rows, span, 128, dtype=F32),
        "ex": vm(rows, span, 128, dtype=F32),
        "core_in": vm(NY, nx, nz // NY, per_sp, 256),
        "x_out": vm(NY, nx, nz // NY, per_sp, 256),
        "x_in": vm(NY, nx, nz // NY, per_sp, 256),
        "last_out": vm(nz, per_sp, 256),
        "last_in": vm(nz, per_sp, 256),
        "ends": vm(rows, 128, dtype=F32),
        "load_sem": sem((15,)),
        "own_sem": sem((2,)),
        "sent": sem((6,)),
        "f_sent": sem((3,)),
    }
    for name in ("send_sem", "ring_sem", "back_sem", "home_sem", "ret_sem", "tg_sem", "p1", "p2", "p3", "g3", "full_sem", "core_sem", "x_sem", "f1", "f2", "f3"):
        scratch[name] = sem
    for name in ("come", "from_l", "from_r", "far_l", "far_r", "a_l", "a_r", "b_l", "b_r"):
        scratch[name] = sem((nz,))
    for name in ("t_l", "t_r", "u_l", "u_r", "g1", "g2"):
        scratch[name] = sem((8,))
    names = ins + list(outs) + list(scratch)

    def body(*refs):
        r = Refs()
        for name, ref in zip(names, refs):
            setattr(r, name, ref)
        mega_kernel(r, nz, nx)

    return pl.pallas_call(
        body,
        name="mega",
        out_shape=tuple(pltpu.VMEM(*kind) for kind in outs.values()),
        in_specs=[pl.BlockSpec(memory_space=pltpu.HBM)] * 13,
        out_specs=(VMEM,) * 8,
        scratch_shapes=list(scratch.values()),
        compiler_params=params(1),
    )(ids, weights, moe, cot, gate, up, down, out_weight, mix, query, key, value, log_decay)


def finish_kernel(*refs):
    count = (len(refs) - 1) // 2
    sem = refs[-1]
    copies = [
        pltpu.make_async_copy(refs[i], refs[count + i], sem.at[i]) for i in range(count)
    ]
    for copy in copies:
        copy.start()
    for copy in copies:
        copy.wait()


def finish(arrays):
    shapes = tuple(jax.ShapeDtypeStruct(a.shape, a.dtype) for a in arrays)
    return pl.pallas_call(
        finish_kernel,
        name="finish",
        out_shape=shapes,
        in_specs=[VMEM] * len(arrays),
        out_specs=(ANY,) * len(arrays),
        scratch_shapes=[pltpu.SemaphoreType.DMA((len(arrays),))],
        compiler_params=pltpu.CompilerParams(vmem_limit_bytes=1024 * 1024),
    )(*[pltpu.with_memory_space_constraint(a, pltpu.VMEM) for a in arrays])


def shards(
    moe_input,
    cotangent,
    expert_ids,
    route_weights,
    gate_weight,
    up_weight,
    down_weight,
    out_weight,
    mixer_out,
    query_vectors,
    key_vectors,
    value_vectors,
    log_decay,
):
    results = mega(
        expert_ids.T,
        route_weights.T,
        moe_input,
        cotangent,
        gate_weight[0],
        up_weight[0],
        down_weight[0],
        out_weight,
        mixer_out,
        query_vectors,
        key_vectors,
        value_vectors,
        log_decay,
    )
    g_gate, g_up, g_down, gout, dq, dk, dv, dl = finish(results)
    return g_gate[None], g_up[None], g_down[None], gout, dq, dk, dv, dl


def solution(mesh):
    finer = Mesh(mesh.devices.reshape(8, 4, 2, mesh.shape["tp"]), ("sp_0", "sp_1", "sp_2", "tp"))
    in_specs = (
        P(SP, None),
        P(SP, None),
        P(SP, None),
        P(SP, None),
        P(SP, None, "tp"),
        P(SP, None, "tp"),
        P(SP, "tp", None),
        P(None, "tp"),
        P(SP, "tp"),
        P(SP, "tp"),
        P(SP, "tp"),
        P(SP, "tp"),
        P(SP, "tp"),
    )
    out_specs = (
        P(SP, None, "tp"),
        P(SP, None, "tp"),
        P(SP, "tp", None),
        P(SP, "tp"),
        P(SP, "tp"),
        P(SP, "tp"),
        P(SP, "tp"),
        P(SP, "tp"),
    )
    return jax.shard_map(
        shards, mesh=finer, in_specs=in_specs, out_specs=out_specs, check_vma=False
    )
```
